128 devices in a mesh: sp: 16 (over z, x), tp: 8 (over y, core).
Axes of the slice: x: 4, y: 4, z: 4, core: 2. Of those that a mesh axis runs over, the one named last changes fastest.
Arguments:
- residual: bfloat16 [8192, 2048], P(('sp', 'tp')), may hold values from -6 to 6
- receptance_first: bfloat16 [8192, 1024], P('sp', 'tp'), may hold values from -6 to 6
- key_first_group: bfloat16 [8192, 1024], P('sp', 'tp'), may hold values from -6 to 6
- value_first_group: bfloat16 [8192, 1024], P('sp', 'tp'), may hold values from -6 to 6
- decay_preact_first: bfloat16 [8192, 1024], P('sp', 'tp'), may hold values from -5.5 to 5.5
- context_rate_first: bfloat16 [8192, 1024], P('sp', 'tp'), may hold values from -6 to 6
- decay_base_first: float32 [1024], P('tp'), may hold values from 9.9e-07 to 0.0301
- head_scale_first: float32 [1024], P('tp'), may hold values from 0.1 to 1.9
- receptance_second: bfloat16 [8192, 1024], P('sp', 'tp'), may hold values from -6 to 6
- key_second_group: bfloat16 [8192, 1024], P('sp', 'tp'), may hold values from -6 to 6
- value_second_group: bfloat16 [8192, 1024], P('sp', 'tp'), may hold values from -6 to 6
- decay_preact_second: bfloat16 [8192, 1024], P('sp', 'tp'), may hold values from -5.5 to 5.5
- context_rate_second: bfloat16 [8192, 1024], P('sp', 'tp'), may hold values from -6 to 6
- decay_base_second: float32 [1024], P('tp'), may hold values from 9.9e-07 to 0.0301
- head_scale_second: float32 [1024], P('tp'), may hold values from 0.1 to 1.9
- decay_extra_log: float32 [8192], P('sp'), may hold values from -0.7 to 0
- output_weight_first: bfloat16 [1024, 2048], P('tp'), may hold values from -0.125 to 0.125
- output_weight_second: bfloat16 [1024, 2048], P('tp'), may hold values from -0.125 to 0.125
- feedforward_gain: float32 [2048], replicated, may hold values from 0.1 to 1.9
- routed_expert_index: int32 [8192, 4], P(('sp', 'tp')), may hold values from 0 to 127, all different within a row; in each aligned block of 64 rows (0 to 63, 64 to 127, ...) at most 4 rows name the same one
- routed_expert_weight: float32 [8192, 4], P(('sp', 'tp')), may hold values from 0.2 to 1
- expert_gate_weight: bfloat16 [128, 2048, 512], P(('sp', 'tp')), may hold values from -0.125 to 0.125
- expert_up_weight: bfloat16 [128, 2048, 512], P(('sp', 'tp')), may hold values from -0.125 to 0.125
- expert_down_weight: bfloat16 [128, 512, 2048], P(('sp', 'tp')), may hold values from -0.25 to 0.25
- shared_gate_weight: bfloat16 [2048, 512], replicated, may hold values from -0.125 to 0.125
- shared_up_weight: bfloat16 [2048, 512], replicated, may hold values from -0.125 to 0.125
- shared_down_weight: bfloat16 [512, 2048], replicated, may hold values from -0.25 to 0.25
Outputs:
- layer_out: bfloat16 [8192, 2048], P(('sp', 'tp'))
The draws below stay inside these ranges and needn't reach their ends.
Inputs may be any that keep to these rules, and one draw needn't show every extreme that they name: `routed_expert_index`: each row names 4 different experts. In each aligned block of the rows of one device, no expert is named by more than 4 rows, a bound that some block reaches.
All inputs are finite; a program needn't handle non-finite values.
Results may differ from the reference program's by a relative error of at most 0.013.
Values may be sent and summed in bfloat16 or wider, within the bound.
A program may use at most 128 MiB of HBM per device.

```python
import math
import jax
import jax.numpy as jnp
import numpy as np
from jax import lax

D = 2048
HEADS_A = 16
HEAD_SIZE_FIRST = 64
HEADS_B = 8
HEAD_SIZE_SECOND = 128
DA = 1024
DB = 1024
EFF = 512
SFF = 512
TOPK = 4
EXPERTS = 128
TOK_DEV = 512
TOKENS = 8192
CAP = 4
N_TP = 8


def shifted_input(key, col_count):
    noise_key = jax.random.fold_in(key, 101)
    shift_key = jax.random.fold_in(key, 102)
    noise_part = jnp.clip(jax.random.normal(noise_key, (TOKENS, col_count), jnp.float32), -4.0, 4.0)
    shifts = jax.random.uniform(shift_key, (TOKENS // TOK_DEV, 1), jnp.float32, -1.5, 1.5)
    return (noise_part + jnp.repeat(shifts, TOK_DEV, axis=0)).astype(jnp.bfloat16)


def rate_table(key, col_count):
    low_log = math.log(1e-06)
    high_log = math.log(0.03)
    return jnp.clip(jnp.exp(jax.random.uniform(jax.random.fold_in(key, 204), (col_count,), jnp.float32, low_log, high_log)), 1e-06, 0.03)


def draw_decay_preact_first(key, part):
    return shifted_input(key, DA)


def draw_decay_preact_second(key, part):
    return shifted_input(key, DB)


def draw_decay_base_first(key, part):
    return rate_table(key, DA)


def draw_decay_base_second(key, part):
    return rate_table(key, DB)


def draw_decay_extra_log(key, part):
    places = jax.random.randint(jax.random.fold_in(key, 301), (6,), 0, TOKENS)
    depths = jnp.log(jax.random.uniform(jax.random.fold_in(key, 302), (6,), jnp.float32, 0.5, 0.8))
    return jnp.zeros((TOKENS,), jnp.float32).at[places].set(depths)


def shard_levels(own_key, shape, cuts, low, largest):
    loudness, own = 1.0, jax.random.fold_in(own_key, 6)
    for dim, parts in cuts:
        draws = jnp.exp(jax.random.uniform(jax.random.fold_in(own, dim), (parts,), jnp.float32, low / len(cuts), largest / len(cuts)))
        loudness = loudness * jnp.repeat(draws, shape[dim] // parts).reshape([-1 if axis == dim else 1 for axis in range(len(shape))])
    return loudness


def routed_block(rng, own, number, rows, count, top, most, skew):
    sequence = jax.random.permutation(rng, count)
    crowded, ordinary = shares(count, rows * top, most, skew, True), shares(count, rows * top, most, skew, False)
    places = jnp.arange(count)

    def named(sizes, rotation):
        used = int((sizes > 0).sum())
        fixed = max(1, used // 4)
        passed = fixed + (places - fixed + rotation * (used - fixed)) % max(1, count - fixed)
        return jnp.zeros((count,), jnp.int32).at[sequence[jnp.where(places < fixed, places, passed)]].set(jnp.asarray(sizes, jnp.int32))

    sizes = jnp.where(number % 4 == 0, named(crowded, number // 4), named(ordinary, number - number // 4 - 1))
    mixed = jax.random.permutation(jax.random.fold_in(own, 3), count)
    giver, receiver = mixed[0:count // 2 * 2:2], mixed[1:count // 2 * 2:2]
    slack = jnp.minimum(sizes[giver] - 1, most - sizes[receiver]) // 2
    slack = jnp.where((giver == sequence[0]) | (receiver == sequence[0]) | (sizes[receiver] == 0), 0, jnp.maximum(slack, 0))
    passed = jax.random.randint(jax.random.fold_in(own, 4), (count // 2,), 0, 1 << 20) % (slack + 1)
    sizes = sizes.at[giver].add(-passed).at[receiver].add(passed)
    labels = jnp.searchsorted(jnp.cumsum(sizes), jnp.arange(rows * top), side="right").astype(jnp.int32)
    grid = labels.reshape(top, rows).T
    grid = grid[jax.random.permutation(jax.random.fold_in(own, 1), rows)]
    rotation = jax.random.randint(jax.random.fold_in(own, 2), (rows, 1), 0, top)
    return jnp.take_along_axis(grid, (jnp.arange(top)[None, :] + rotation) % top, axis=1)


def shares(count, total, most, skew, full):
    weights = [(1 << 20) // math.isqrt(rank ** skew) + 1 for rank in range(1, count + 1)]
    largest = most if full else min(most, max(-(-total // count), total * weights[0] // sum(weights)))
    least = 1 if total - largest >= count - 1 else 0
    given, surplus = [largest] + [least] * (count - 1), total - largest - least * (count - 1)
    while surplus > 0:
        movable = [i for i in range(1, count) if given[i] < largest] or [i for i in range(1, count) if given[i] < most]
        whole, remaining = sum([weights[i] for i in movable]), surplus
        for i in movable:
            more = min(most - given[i], max(1, remaining * weights[i] // whole), surplus)
            given[i] = given[i] + more
            surplus = surplus - more
    return np.array(given)


def normal_values(stream_key, extent, deviation, reach, split=(), kind=jnp.bfloat16):
    array = deviation * jax.random.normal(stream_key, extent, jnp.float32)
    if split:
        array = array * shard_levels(stream_key, extent, split, -0.22, 0.18)
    return jnp.clip(array, -reach, reach).astype(kind)


def setup_inputs(seed: int = 0) -> dict:
    key_list = jax.random.split(jax.random.key(seed), 28)
    residual = normal_values(key_list[0], (TOKENS, D), 1.0, 6.0, ((0, 128),))
    receptance_first = normal_values(key_list[1], (TOKENS, DA), 1.0, 6.0, ((0, 16), (1, 8)))
    key_first_group = normal_values(key_list[2], (TOKENS, DA), 1.0, 6.0, ((0, 16), (1, 8)))
    value_first_group = normal_values(key_list[3], (TOKENS, DA), 1.0, 6.0, ((0, 16), (1, 8)))
    decay_preact_first = draw_decay_preact_first(jax.random.fold_in(key_list[27], 71), 0)
    context_rate_first = normal_values(key_list[5], (TOKENS, DA), 1.5, 6.0, ((0, 16), (1, 8)))
    decay_base_first = draw_decay_base_first(jax.random.fold_in(key_list[27], 71), 0)
    head_scale_first = jnp.clip(1.0 + 0.18 * jax.random.normal(key_list[7], (DA,), jnp.float32), 0.1, 1.9)
    receptance_second = normal_values(key_list[8], (TOKENS, DB), 1.0, 6.0, ((0, 16), (1, 8)))
    key_second_group = normal_values(key_list[9], (TOKENS, DB), 1.0, 6.0, ((0, 16), (1, 8)))
    value_second_group = normal_values(key_list[10], (TOKENS, DB), 1.0, 6.0, ((0, 16), (1, 8)))
    decay_preact_second = draw_decay_preact_second(jax.random.fold_in(key_list[27], 71), 0)
    context_rate_second = normal_values(key_list[12], (TOKENS, DB), 1.5, 6.0, ((0, 16), (1, 8)))
    decay_base_second = draw_decay_base_second(jax.random.fold_in(key_list[27], 71), 0)
    head_scale_second = jnp.clip(1.0 + 0.18 * jax.random.normal(key_list[14], (DB,), jnp.float32), 0.1, 1.9)
    decay_extra_log = draw_decay_extra_log(jax.random.fold_in(key_list[27], 71), 0)
    output_weight_first = normal_values(key_list[16], (DA, D), (DA + DB) ** -0.5, 0.125, ((0, 8),))
    output_weight_second = normal_values(key_list[17], (DB, D), (DA + DB) ** -0.5, 0.125, ((0, 8),))
    feedforward_gain = jnp.clip(1.0 + 0.18 * jax.random.normal(key_list[18], (D,), jnp.float32), 0.1, 1.9)
    routed_expert_index_keys = jax.random.split(jax.random.fold_in(key_list[19], 1), TOKENS // (TOK_DEV // N_TP))
    routed_expert_index_turns = jax.random.permutation(jax.random.fold_in(key_list[19], 3), TOKENS // (TOK_DEV // N_TP))
    routed_expert_index = jax.vmap(lambda own, number: routed_block(jax.random.fold_in(key_list[19], 2), own, number, TOK_DEV // N_TP, EXPERTS, TOPK, CAP, 2))(routed_expert_index_keys, routed_expert_index_turns).reshape((TOKENS, TOPK))
    routed_expert_weight = jnp.clip(0.2 + 0.8 * jax.random.uniform(key_list[20], (TOKENS, TOPK), jnp.float32) ** shard_levels(key_list[20], (TOKENS, TOPK), ((0, 128),), -0.2, 0.2), 0.2, 1.0)
    expert_gate_weight = normal_values(key_list[21], (EXPERTS, D, EFF), D ** -0.5, 0.125, ((0, 128),))
    expert_up_weight = normal_values(key_list[22], (EXPERTS, D, EFF), D ** -0.5, 0.125, ((0, 128),))
    expert_down_weight = normal_values(key_list[23], (EXPERTS, EFF, D), EFF ** -0.5, 0.25, ((0, 128),))
    shared_gate_weight = normal_values(key_list[24], (D, SFF), D ** -0.5, 0.125)
    shared_up_weight = normal_values(key_list[25], (D, SFF), D ** -0.5, 0.125)
    shared_down_weight = normal_values(key_list[26], (SFF, D), SFF ** -0.5, 0.25)
    return {"residual": residual, "receptance_first": receptance_first, "key_first_group": key_first_group, "value_first_group": value_first_group, "decay_preact_first": decay_preact_first, "context_rate_first": context_rate_first, "decay_base_first": decay_base_first, "head_scale_first": head_scale_first, "receptance_second": receptance_second, "key_second_group": key_second_group, "value_second_group": value_second_group, "decay_preact_second": decay_preact_second, "context_rate_second": context_rate_second, "decay_base_second": decay_base_second, "head_scale_second": head_scale_second, "decay_extra_log": decay_extra_log, "output_weight_first": output_weight_first, "output_weight_second": output_weight_second, "feedforward_gain": feedforward_gain, "routed_expert_index": routed_expert_index, "routed_expert_weight": routed_expert_weight, "expert_gate_weight": expert_gate_weight, "expert_up_weight": expert_up_weight, "expert_down_weight": expert_down_weight, "shared_gate_weight": shared_gate_weight, "shared_up_weight": shared_up_weight, "shared_down_weight": shared_down_weight}


NORM_EPSILON = 1e-06
HEAD_EPSILON = 0.00064
KEY_EPSILON = 1e-06
PRECISE = lax.Precision.HIGHEST

def head_pieces_list(receptance_rows, key_row_block, value_rows, decay_preact, context_rate_preact, decay_base_rate, decay_extra_log, head_width_value):

    def arrange(source):
        return source.astype(jnp.float32).reshape(source.shape[0], -1, head_width_value)
    raw_keys = arrange(key_row_block)
    unit_key = raw_keys * lax.rsqrt(lax.optimization_barrier(jnp.sum(raw_keys * raw_keys, axis=-1, keepdims=True)) + KEY_EPSILON)
    removal = unit_key * jax.nn.sigmoid(arrange(context_rate_preact))
    logarithm_decay = decay_extra_log.astype(jnp.float32)[:, None] - 2.0 * decay_base_rate.astype(jnp.float32)[None, :] * jax.nn.sigmoid(decay_preact.astype(jnp.float32))
    return (arrange(receptance_rows), jnp.exp(arrange(logarithm_decay)), unit_key, removal, arrange(value_rows))

def advance(state_mat, unit_key, removal, value_rows, decay_now, receptance_rows):
    erased = value_rows - jnp.einsum('hvk,hk->hv', state_mat, unit_key, precision=PRECISE)
    state_mat = state_mat * decay_now[:, None, :] + erased[:, :, None] * removal[:, None, :]
    return (state_mat, jnp.einsum('hvk,hk->hv', state_mat, receptance_rows, precision=PRECISE))

def head_norm(readout, head_gain):
    centre = lax.optimization_barrier(jnp.mean(readout, axis=-1, keepdims=True))
    centered = readout - centre
    spread = lax.optimization_barrier(jnp.mean(centered * centered, axis=-1, keepdims=True))
    flattened = (centered * lax.rsqrt(spread + HEAD_EPSILON)).reshape(readout.shape[0], -1)
    return (flattened * head_gain.astype(jnp.float32)).astype(jnp.bfloat16)

def swiglu_hidden(inputs, w_gate, w_up):
    gate_val = jnp.dot(inputs, w_gate, preferred_element_type=jnp.float32)
    up_val = jnp.dot(inputs, w_up, preferred_element_type=jnp.float32)
    return (jax.nn.silu(gate_val) * up_val).astype(jnp.bfloat16)

def reference(residual, receptance_first, key_first_group, value_first_group, decay_preact_first, context_rate_first, decay_base_first, head_scale_first, receptance_second, key_second_group, value_second_group, decay_preact_second, context_rate_second, decay_base_second, head_scale_second, decay_extra_log, output_weight_first, output_weight_second, feedforward_gain, routed_expert_index, routed_expert_weight, expert_gate_weight, expert_up_weight, expert_down_weight, shared_gate_weight, shared_up_weight, shared_down_weight):
    pieces_first = head_pieces_list(receptance_first, key_first_group, value_first_group, decay_preact_first, context_rate_first, decay_base_first, decay_extra_log, HEAD_SIZE_FIRST)
    pieces_second = head_pieces_list(receptance_second, key_second_group, value_second_group, decay_preact_second, context_rate_second, decay_base_second, decay_extra_log, HEAD_SIZE_SECOND)

    def advance_both(carried, inputs):
        state_a, state_b = carried
        state_a, read_a = advance(state_a, inputs[2], inputs[3], inputs[4], inputs[1], inputs[0])
        state_b, read_b = advance(state_b, inputs[7], inputs[8], inputs[9], inputs[6], inputs[5])
        return ((state_a, state_b), (read_a, read_b))
    initial = (jnp.zeros((HEADS_A, HEAD_SIZE_FIRST, HEAD_SIZE_FIRST), jnp.float32), jnp.zeros((HEADS_B, HEAD_SIZE_SECOND, HEAD_SIZE_SECOND), jnp.float32))
    _, (read_a, read_b) = lax.scan(advance_both, initial, pieces_first + pieces_second)
    mixed_a = head_norm(read_a, head_scale_first)
    mixed_b = head_norm(read_b, head_scale_second)
    projected = jnp.dot(mixed_a, output_weight_first, preferred_element_type=jnp.float32) + jnp.dot(mixed_b, output_weight_second, preferred_element_type=jnp.float32)
    attended = (residual.astype(jnp.float32) + projected).astype(jnp.bfloat16)
    attended_f = attended.astype(jnp.float32)
    normed = (attended_f * lax.rsqrt(lax.optimization_barrier(jnp.mean(attended_f * attended_f, axis=-1, keepdims=True)) + NORM_EPSILON) * feedforward_gain.astype(jnp.float32)).astype(jnp.bfloat16)
    shared_out = jnp.dot(swiglu_hidden(normed, shared_gate_weight, shared_up_weight), shared_down_weight, preferred_element_type=jnp.float32)
    assigned = TOKENS * TOPK
    flat_ids = routed_expert_index.reshape(-1).astype(jnp.int32)
    token_of = jnp.concatenate([jnp.arange(assigned, dtype=jnp.int32) // TOPK, jnp.full((1,), TOKENS, jnp.int32)])
    weight_of = jnp.concatenate([routed_expert_weight.reshape(-1).astype(jnp.float32), jnp.zeros((1,), jnp.float32)])
    row_limit = TOKENS // (TOK_DEV // N_TP) * CAP
    padded = jnp.concatenate([normed, jnp.zeros((1, D), jnp.bfloat16)], axis=0)

    def one_expert(summed, expert):
        chosen = jnp.nonzero(flat_ids == expert, size=row_limit, fill_value=assigned)[0].astype(jnp.int32)
        owners = token_of[chosen]
        hidden = swiglu_hidden(padded[owners], expert_gate_weight[expert], expert_up_weight[expert])
        result = jnp.dot(hidden, expert_down_weight[expert], preferred_element_type=jnp.float32).astype(jnp.bfloat16)
        return (summed.at[owners].add(result.astype(jnp.float32) * weight_of[chosen][:, None]), None)
    routed, _ = lax.scan(one_expert, jnp.zeros((TOKENS + 1, D), jnp.float32), jnp.arange(EXPERTS, dtype=jnp.int32))
    return (attended_f + shared_out + routed[:TOKENS]).astype(jnp.bfloat16)
```

```python
import functools
import jax
import jax.numpy as jnp
from jax import lax
from jax.experimental import pallas as pl
from jax.experimental.pallas import tpu as pltpu
from jax.sharding import Mesh
from jax.sharding import PartitionSpec as P

F32, BF16 = jnp.float32, jnp.bfloat16
SPAN = 128
LANES = 128
KEY_EPSILON = 1e-06
HEAD_EPSILON = 0.00064
NORM_EPSILON = 1e-06


def nn(a, b):
    return lax.dot_general(a, b, (((1,), (0,)), ((), ())), preferred_element_type=F32)


def nt(a, b):
    return lax.dot_general(a, b, (((1,), (1,)), ((), ())), preferred_element_type=F32)


def halves(x):
    high = x.astype(BF16)
    return high, (x - high.astype(F32)).astype(BF16)


def dot1(f, a, b):
    return f(a.astype(BF16), b.astype(BF16))


def dot3(f, a, b):
    ah, al = halves(a)
    bh, bl = halves(b)
    return f(ah, bh) + (f(ah, bl) + f(al, bh))


def iota(shape, dim):
    return lax.broadcasted_iota(jnp.int32, shape, dim)


def head_sum(x, width):
    if width == LANES:
        return jnp.sum(x, axis=-1, keepdims=True)
    lane = iota(x.shape, 1)
    left = jnp.sum(jnp.where(lane < width, x, 0.0), axis=-1, keepdims=True)
    right = jnp.sum(jnp.where(lane < width, 0.0, x), axis=-1, keepdims=True)
    return jnp.where(lane < width, left, right)


def local_kernel(dot, *refs):
    (r_a, k_a, v_a, p_a, c_a, base_a, r_b, k_b, v_b, p_b, c_b, base_b, extra_ref) = refs[:13]
    read_a, map_a, read_b, map_b, message = refs[13:]
    square = (SPAN, SPAN)
    row, col = iota(square, 0), iota(square, 1)
    lower = row >= col
    strict = row > col
    lower_bf = jnp.where(lower, 1.0, 0.0).astype(BF16)
    eye = jnp.where(row == col, 1.0, 0.0)
    count = r_a.shape[0] // SPAN
    items = []
    for group, (r_, k_, v_, p_, c_, base_, width) in enumerate(
        ((r_a, k_a, v_a, p_a, c_a, base_a, 64), (r_b, k_b, v_b, p_b, c_b, base_b, 128))
    ):
        for block in range(count):
            at = pl.ds(block * SPAN, SPAN)
            key = k_[at, :].astype(F32)
            unit = key * lax.rsqrt(head_sum(key * key, width) + KEY_EPSILON)
            removal = unit * jax.nn.sigmoid(c_[at, :].astype(F32))
            slow = jax.nn.sigmoid(p_[at, :].astype(F32))
            extra = extra_ref[pl.ds(block, 1), :]
            rate = 2.0 * base_[...]
            high, low = halves(slow)
            run_slow = nn(lower_bf, high) + nn(lower_bf, low)
            run_extra = jnp.sum(jnp.where(lower, extra, 0.0), axis=-1, keepdims=True)
            own_extra = jnp.sum(jnp.where(row == col, extra, 0.0), axis=-1, keepdims=True)
            running = run_extra - rate * run_slow
            own_log = own_extra - rate * slow
            centre = running[SPAN // 2 - 1 : SPAN // 2, :]
            ending = running[SPAN - 1 : SPAN, :]
            grown = running - centre
            read = r_[at, :].astype(F32) * jnp.exp(grown)
            query = unit * jnp.exp(grown - own_log)
            write = removal * jnp.exp(-grown)
            write_end = write * jnp.exp(ending - centre)
            items.append(
                dict(
                    group=group,
                    block=block,
                    width=width,
                    read=read,
                    query=query,
                    write=write,
                    write_end=write_end,
                    value=v_[at, :].astype(F32),
                    centre=jnp.exp(centre),
                    ending=jnp.exp(ending),
                )
            )
    solves = []
    for item in items:
        lane = col < item["width"]
        masks = [None] if item["width"] == SPAN else [lane, jnp.logical_not(lane)]
        item["parts"] = []
        for mask in masks:
            query = item["query"] if mask is None else jnp.where(mask, item["query"], 0.0)
            read = item["read"] if mask is None else jnp.where(mask, item["read"], 0.0)
            both = dot(nt, jnp.concatenate([query, read], axis=0), item["write"])
            coupling = jnp.where(strict, both[:SPAN], 0.0)
            reading = jnp.where(lower, both[SPAN:], 0.0)
            part = dict(mask=mask, coupling=coupling, reading=reading)
            item["parts"].append(part)
            solves.append(part)
    size = 1
    while size < SPAN:
        near = ((row // (2 * size)) == (col // (2 * size))) & ((row // size) > (col // size))
        for part in solves:
            step = jnp.where(near, part["coupling"], 0.0)
            if size == 1:
                part["inverse"] = eye - step
            else:
                inverse = part["inverse"]
                part["inverse"] = inverse - dot(nn, dot(nn, inverse, step), inverse)
        size *= 2
    head_row, head_col = row < 64, col < 64
    same_head = head_row == head_col
    for item in items:
        parts = item["parts"]
        right = jnp.concatenate([item["value"], -item["query"]], axis=1)
        wide = iota(right.shape, 1) % SPAN < 64

        def spread(x):
            if len(parts) == 1:
                return x
            return jnp.concatenate([jnp.where(wide, x, 0.0), jnp.where(wide, 0.0, x)], axis=0)

        def joined(name):
            return jnp.concatenate([part[name] for part in parts], axis=1)

        solved = dot(nn, joined("inverse"), spread(right))
        given = dot(nn, joined("reading"), spread(solved))
        item["local_read"] = given[:, :SPAN]
        item["state_read"] = (item["read"] + given[:, SPAN:]) * item["centre"]
        scaled = jnp.concatenate([solved[:, :SPAN], solved[:, SPAN:] * item["centre"]], axis=1)
        step = dot(nn, item["write_end"].T, scaled)
        diagonal = jnp.where(row == col, item["ending"], 0.0)
        step = step + jnp.concatenate([jnp.zeros(square, F32), diagonal], axis=1)
        if item["width"] < SPAN:
            both_heads = jnp.concatenate([same_head, same_head], axis=1)
            step = jnp.where(both_heads, step, 0.0)
        item["step"] = step
    for group, (read_ref, map_ref) in enumerate(((read_a, map_a), (read_b, map_b))):
        held = None
        for item in items:
            if item["group"] != group:
                continue
            at = pl.ds(item["block"] * SPAN, SPAN)
            if held is None:
                read_ref[at, :] = item["local_read"]
                map_ref[at, :] = item["state_read"].astype(BF16)
                held = item["step"]
            else:
                out = dot(nn, item["state_read"], held)
                read_ref[at, :] = item["local_read"] + out[:, :SPAN]
                map_ref[at, :] = out[:, SPAN:].astype(BF16)
                step = item["step"]
                held = dot(nn, step[:, SPAN:], held)
                held = jnp.concatenate([held[:, :SPAN] + step[:, :SPAN], held[:, SPAN:]], axis=1)
        if group == 0:
            message[0:64, :] = (held[:64, :] + held[64:, :]).astype(BF16)
        else:
            message[64:192, :] = held.astype(BF16)


def local_call(args, dot=dot1):
    rows = args[0].shape[0]
    shapes = [
        jax.ShapeDtypeStruct((rows, LANES), F32),
        jax.ShapeDtypeStruct((rows, LANES), BF16),
        jax.ShapeDtypeStruct((rows, LANES), F32),
        jax.ShapeDtypeStruct((rows, LANES), BF16),
        jax.ShapeDtypeStruct((192, 2 * LANES), BF16),
    ]
    return pl.pallas_call(
        functools.partial(local_kernel, dot),
        out_shape=shapes,
        in_specs=[pl.BlockSpec(memory_space=pltpu.VMEM)] * 13,
        out_specs=[pl.BlockSpec(memory_space=pltpu.VMEM)] * 5,
        name="local_terms",
    )(*args)


Z, X, Y, C = "z", "x", "y", "core"
ALL = (Z, X, Y, C)
MESH = pl.DeviceIdType.MESH
VMEM = pltpu.VMEM


def whole(count):
    return [pl.BlockSpec(memory_space=pltpu.VMEM)] * count


def greet(peers):
    barrier = pltpu.get_barrier_semaphore()
    for peer in peers:
        pl.semaphore_signal(barrier, inc=1, device_id=peer, device_id_type=MESH)
    pl.semaphore_wait(barrier, len(peers))


def follow(step, held):
    high, low = halves(held)
    moved = nn(step[:, LANES:], high) + nn(step[:, LANES:], low)
    return moved


def exchange_kernel(
    message, enter_a, enter_b, rows, columns, total, row_send, row_recv, col_send, col_recv
):
    z, x, y, c = [lax.axis_index(name) for name in ALL]
    row_peers = [(z, lax.rem(x + d, 4), y, c) for d in range(1, 4)]
    col_peers = [(lax.rem(z + d, 4), x, y, c) for d in range(1, 4)]
    greet(row_peers + col_peers)

    def row_copy(d):
        return pltpu.make_async_remote_copy(
            src_ref=message,
            dst_ref=rows.at[d],
            send_sem=row_send.at[d],
            recv_sem=row_recv.at[d],
            device_id=row_peers[d - 1],
            device_id_type=MESH,
        )

    def col_copy(d):
        return pltpu.make_async_remote_copy(
            src_ref=total,
            dst_ref=columns.at[d],
            send_sem=col_send.at[d],
            recv_sem=col_recv.at[d],
            device_id=col_peers[d - 1],
            device_id_type=MESH,
        )

    for d in (2, 1, 3):
        row_copy(d).start()
    rows[0] = message[...]
    square = (LANES, 2 * LANES)
    row, col = iota(square, 0), iota(square, 1)
    same = (row < 64) == (col % LANES < 64)
    unit = jnp.where(row + LANES == col, 1.0, 0.0)
    for d in range(1, 4):
        row_copy(d).wait()

    def steps(packed):
        top = packed[0:64, :]
        first = jnp.where(same, jnp.concatenate([top, top], axis=0), jnp.zeros((), BF16))
        return first, packed[64:192, :]

    def chain(step, held):
        moved = follow(step, held)
        own = step[:, :LANES].astype(F32)
        return jnp.concatenate([moved[:, :LANES] + own, moved[:, LANES:]], axis=1)

    inside = [unit, unit]
    running = [unit, unit]
    for k in range(4):
        pair = steps(rows[lax.rem(x - k + 4, 4)])
        inside = [jnp.where(x == k, now, old) for now, old in zip(running, inside)]
        if k == 0:
            running = [p.astype(F32) for p in pair]
        else:
            running = [chain(p, r) for p, r in zip(pair, running)]
    total[0:64, :] = (running[0][:64, :] + running[0][64:, :]).astype(BF16)
    total[64:192, :] = running[1].astype(BF16)
    for d in (2, 1, 3):

        @pl.when(z + d < 4)
        def _():
            col_copy(d).start()

    enter_a[...] = jnp.zeros_like(enter_a)
    enter_b[...] = jnp.zeros_like(enter_b)
    for k in range(3):

        @pl.when(k < z)
        def _():
            d = z - k
            pltpu.make_async_remote_copy(
                src_ref=total,
                dst_ref=columns.at[d],
                send_sem=col_send.at[d],
                recv_sem=col_recv.at[d],
                device_id=(k, x, y, c),
                device_id_type=MESH,
            ).wait_recv()
            pair = steps(columns[d])
            for enter, step in zip((enter_a, enter_b), pair):
                enter[...] = follow(step, enter[...]) + step[:, :LANES].astype(F32)

    for enter, own in zip((enter_a, enter_b), inside):
        enter[...] = dot3(nn, own[:, LANES:], enter[...]) + own[:, :LANES]
    for d in (2, 1, 3):

        @pl.when(z + d < 4)
        def _():
            col_copy(d).wait_send()


def exchange_call(message):
    shape = jax.ShapeDtypeStruct((LANES, LANES), F32)
    return pl.pallas_call(
        exchange_kernel,
        out_shape=[shape, shape],
        in_specs=whole(1),
        out_specs=whole(2),
        scratch_shapes=[
            pltpu.VMEM((4, 192, 2 * LANES), BF16),
            pltpu.VMEM((4, 192, 2 * LANES), BF16),
            pltpu.VMEM((192, 2 * LANES), BF16),
        ]
        + [pltpu.SemaphoreType.DMA((4,))] * 4,
        compiler_params=pltpu.CompilerParams(collective_id=1, has_side_effects=True),
        name="exchange",
    )(message)


def project_kernel(
    read_a, map_a, enter_a, gain_a, weight_a, read_b, map_b, enter_b, gain_b, weight_b, out
):
    square = (LANES, LANES)
    row, col = iota(square, 0), iota(square, 1)
    mixed = []
    for read, map_, enter, gain, width in (
        (read_a, map_a, enter_a, gain_a, 64),
        (read_b, map_b, enter_b, gain_b, 128),
    ):
        mean = jnp.where((row // width) == (col // width), 1.0 / width, 0.0).astype(BF16)
        high, low = halves(enter[...])
        readout = read[...] + nn(map_[...], high) + nn(map_[...], low)
        high, low = halves(readout)
        centred = readout - (nn(high, mean) + nn(low, mean))
        high, low = halves(centred * centred)
        spread = nn(high, mean) + nn(low, mean)
        mixed.append((centred * lax.rsqrt(spread + HEAD_EPSILON) * gain[...]).astype(BF16))
    rows, width = out.shape
    both = jnp.concatenate(mixed, axis=1)
    weight = jnp.concatenate([weight_a[...], weight_b[...]], axis=0)
    for at in range(0, width, 512):
        out[:, at : at + 512] = nn(both, weight[:, at : at + 512]).astype(BF16)


def project_call(args, rows, width):
    return pl.pallas_call(
        project_kernel,
        out_shape=jax.ShapeDtypeStruct((rows, width), BF16),
        in_specs=whole(10),
        out_specs=whole(1)[0],
        name="project",
    )(*args)


def scatter_kernel(part, out, pair_in, own, ring_in, pair_send, pair_recv, ring_send, ring_recv):
    z, x, y, c = [lax.axis_index(name) for name in ALL]
    partner = (z, x, y, 1 - c)
    peers = [(z, x, lax.rem(y + d, 4), c) for d in range(1, 4)]
    greet([partner] + peers)
    rows = out.shape[0]

    def pair_copy(d):
        goal = lax.rem(y + d, 4)
        return pltpu.make_async_remote_copy(
            src_ref=part.at[goal * 2 + (1 - c)],
            dst_ref=pair_in.at[d],
            send_sem=pair_send.at[d],
            recv_sem=pair_recv.at[d],
            device_id=partner,
            device_id_type=MESH,
        )

    def ring_copy(d):
        return pltpu.make_async_remote_copy(
            src_ref=own.at[d],
            dst_ref=ring_in.at[d],
            send_sem=ring_send.at[d],
            recv_sem=ring_recv.at[d],
            device_id=peers[d - 1],
            device_id_type=MESH,
        )

    for d in (2, 1, 3, 0):
        pair_copy(d).start()
    for d in (2, 1, 3):
        pair_copy(d).wait()
        goal = lax.rem(y + d, 4)
        own[d] = (part[goal * 2 + c].astype(F32) + pair_in[d].astype(F32)).astype(BF16)
        ring_copy(d).start()
    pair_copy(0).wait()
    out[...] = part[y * 2 + c].astype(F32) + pair_in[0].astype(F32)
    for d in (1, 3, 2):
        ring_copy(d).wait()
        out[...] += ring_in[d].astype(F32)


def scatter_call(part):
    blocks, rows, width = part.shape
    return pl.pallas_call(
        scatter_kernel,
        out_shape=jax.ShapeDtypeStruct((rows, width), F32),
        in_specs=whole(1),
        out_specs=whole(1)[0],
        scratch_shapes=[pltpu.VMEM((4, rows, width), BF16)] * 3
        + [pltpu.SemaphoreType.DMA((4,))] * 4,
        compiler_params=pltpu.CompilerParams(collective_id=2, has_side_effects=True),
        name="scatter_sum",
    )(part)


SLOTS = 4
PARTS = 4
UNIT = SLOTS * PARTS


def routing(index):
    rows, top = index.shape
    experts = iota((rows, LANES), 1)
    chosen = jnp.zeros((rows, LANES), F32)
    for k in range(top):
        chosen += jnp.where(index[:, k : k + 1] == experts, 1.0, 0.0)
    earlier = jnp.where(iota((rows, rows), 0) > iota((rows, rows), 1), 1.0, 0.0).astype(BF16)
    rank = nn(earlier, chosen.astype(BF16))
    code = (chosen * (rank + 1.0)).astype(BF16)
    return jnp.concatenate([code] * PARTS, axis=0)


def dispatch_kernel(residual, summed, gain, index, attended, normed, sent):
    total = (residual[...].astype(F32) + summed[...]).astype(BF16)
    attended[...] = total
    wide = total.astype(F32)
    mean = jnp.mean(wide * wide, axis=-1, keepdims=True)
    rows_ = (wide * lax.rsqrt(mean + NORM_EPSILON) * gain[...]).astype(BF16)
    normed[...] = rows_
    rows, width = rows_.shape
    part = width // PARTS
    stacked = jnp.concatenate([rows_[:, q * part : (q + 1) * part] for q in range(PARTS)], axis=0)
    code = routing(index)
    shape = (256, PARTS * rows)
    place = iota(shape, 0) % UNIT
    fits = (place // SLOTS) == (iota(shape, 1) // rows)
    wanted = (place % SLOTS + 1).astype(F32)
    for k in range(sent.shape[0] // 256):
        select = (iota((256, LANES), 0) + 256 * k) // UNIT == iota((256, LANES), 1)
        found = nt(jnp.where(select, 1.0, 0.0).astype(BF16), code)
        taken = jnp.where(fits & (found == wanted), 1.0, 0.0).astype(BF16)
        sent[256 * k : 256 * (k + 1), :] = nn(taken, stacked).astype(BF16)


def dispatch_call(residual, summed, gain, index, devices):
    rows, width = residual.shape
    return pl.pallas_call(
        dispatch_kernel,
        out_shape=[
            jax.ShapeDtypeStruct((rows, width), BF16),
            jax.ShapeDtypeStruct((rows, width), BF16),
            jax.ShapeDtypeStruct((devices * UNIT, width // PARTS), BF16),
        ],
        in_specs=whole(4),
        out_specs=whole(3),
        name="dispatch",
    )(residual, summed, gain, index)


def expert_kernel(arrived, gate, up, down, out, rows_, hidden):
    part = arrived.shape[1]
    groups = arrived.shape[0] // 256
    a, b = iota((256, 256), 0), iota((256, 256), 1)
    here = (b % UNIT // SLOTS) * 64 + (b // UNIT) * SLOTS + b % SLOTS
    order = jnp.where(a == here, 1.0, 0.0).astype(BF16)
    there = (a % UNIT // SLOTS) * 64 + (a // UNIT) * SLOTS + a % SLOTS
    back = jnp.where(b == there, 1.0, 0.0).astype(BF16)
    for k in range(groups):
        sorted_ = nn(order, arrived[256 * k : 256 * (k + 1), :]).astype(BF16)
        for q in range(PARTS):
            rows_[64 * k : 64 * (k + 1), q * part : (q + 1) * part] = sorted_[64 * q : 64 * (q + 1)]
    for at in range(0, hidden.shape[1], 256):
        gate_val = nn(rows_[...], gate[:, at : at + 256])
        up_val = nn(rows_[...], up[:, at : at + 256])
        hidden[:, at : at + 256] = (gate_val * jax.nn.sigmoid(gate_val) * up_val).astype(BF16)
    for at in range(0, rows_.shape[1], 512):
        rows_[:, at : at + 512] = nn(hidden[...], down[:, at : at + 512]).astype(BF16)
    for k in range(groups):
        stacked = jnp.concatenate(
            [rows_[64 * k : 64 * (k + 1), q * part : (q + 1) * part] for q in range(PARTS)], axis=0
        )
        out[256 * k : 256 * (k + 1), :] = nn(back, stacked).astype(BF16)


def expert_call(arrived, gate, up, down):
    slots = arrived.shape[0] // PARTS
    return pl.pallas_call(
        expert_kernel,
        out_shape=jax.ShapeDtypeStruct(arrived.shape, BF16),
        in_specs=whole(4),
        out_specs=whole(1)[0],
        scratch_shapes=[
            pltpu.VMEM((slots, gate.shape[0]), BF16),
            pltpu.VMEM((slots, gate.shape[1]), BF16),
        ],
        compiler_params=pltpu.CompilerParams(vmem_limit_bytes=60 * 1024 * 1024),
        name="expert",
    )(arrived, gate, up, down)


def combine_kernel(attended, shared, returned, index, weights, out):
    rows, width = attended.shape
    part = width // PARTS
    code = routing(index)
    experts = iota((rows, LANES), 1)
    scale = jnp.zeros((rows, LANES), F32)
    for k in range(index.shape[1]):
        scale += jnp.where(index[:, k : k + 1] == experts, weights[:, k : k + 1], 0.0)
    high, low = halves(jnp.concatenate([scale] * PARTS, axis=0))
    shape = (PARTS * rows, 256)
    place = iota(shape, 1) % UNIT
    fits = (place // SLOTS) == (iota(shape, 0) // rows)
    wanted = (place % SLOTS + 1).astype(F32)
    routed = jnp.zeros((PARTS * rows, part), F32)
    for k in range(returned.shape[0] // 256):
        select = (iota((256, LANES), 0) + 256 * k) // UNIT == iota((256, LANES), 1)
        select = jnp.where(select, 1.0, 0.0).astype(BF16)
        match = fits & (nt(code, select) == wanted)
        block = returned[256 * k : 256 * (k + 1), :]
        routed += nn(jnp.where(match, nt(high, select), 0.0).astype(BF16), block)
        routed += nn(jnp.where(match, nt(low, select), 0.0).astype(BF16), block)
    for q in range(PARTS):
        at = slice(q * part, (q + 1) * part)
        out[:, at] = (
            attended[:, at].astype(F32) + shared[:, at] + routed[q * rows : (q + 1) * rows, :]
        ).astype(BF16)


def combine_call(attended, shared, returned, index, weights):
    return pl.pallas_call(
        combine_kernel,
        out_shape=jax.ShapeDtypeStruct(attended.shape, BF16),
        in_specs=whole(5),
        out_specs=whole(1)[0],
        name="combine",
    )(attended, shared, returned, index, weights)


def swap_kernel(source, out, send, recv, own_sem):
    z, x, y, c = [lax.axis_index(name) for name in ALL]
    me = ((z * 4 + x) * 4 + y) * 2 + c
    devices = source.shape[0] // UNIT

    def block(k):
        return pl.ds(pl.multiple_of(k * UNIT, UNIT), UNIT)

    def copy(d):
        dz, dx, dy, dc = d % 4, d // 4 % 4, d // 16 % 4, d // 64
        pz, px, py, pc = (z + dz) % 4, (x + dx) % 4, (y + dy) % 4, (c + dc) % 2
        peer = ((pz * 4 + px) * 4 + py) * 2 + pc
        sz, sx, sy, sc = (z - dz + 4) % 4, (x - dx + 4) % 4, (y - dy + 4) % 4, (c - dc + 2) % 2
        giver = ((sz * 4 + sx) * 4 + sy) * 2 + sc
        start = pltpu.make_async_remote_copy(
            src_ref=source.at[block(peer)],
            dst_ref=out.at[block(me)],
            send_sem=send.at[d],
            recv_sem=recv.at[d],
            device_id=(pz, px, py, pc),
            device_id_type=MESH,
        )
        arrive = pltpu.make_async_remote_copy(
            src_ref=source.at[block(peer)],
            dst_ref=out.at[block(giver)],
            send_sem=send.at[d],
            recv_sem=recv.at[d],
            device_id=(pz, px, py, pc),
            device_id_type=MESH,
        )
        return start, arrive

    @pl.loop(1, devices)
    def _(d):
        copy(d)[0].start()

    out[block(me), :] = source[block(me), :]

    @pl.loop(1, devices)
    def _(d):
        copy(d)[1].wait()


def swap_call(source):
    devices = source.shape[0] // UNIT
    return pl.pallas_call(
        swap_kernel,
        out_shape=jax.ShapeDtypeStruct(source.shape, BF16),
        in_specs=whole(1),
        out_specs=whole(1)[0],
        scratch_shapes=[pltpu.SemaphoreType.DMA((devices,))] * 2 + [pltpu.SemaphoreType.DMA],
        compiler_params=pltpu.CompilerParams(has_side_effects=True),
        name="swap",
    )(source)


def swiglu_hidden(inputs, w_gate, w_up):
    gate_val = jnp.dot(inputs, w_gate, preferred_element_type=F32)
    up_val = jnp.dot(inputs, w_up, preferred_element_type=F32)
    return (jax.nn.silu(gate_val) * up_val).astype(BF16)


def exchange_slots(slots):
    devices = slots.shape[0] // UNIT
    return lax.all_to_all(
        slots.reshape(devices, UNIT, -1), ALL, split_axis=0, concat_axis=0, tiled=True
    ).reshape(slots.shape)


def local(
    residual,
    receptance_first,
    key_first_group,
    value_first_group,
    decay_preact_first,
    context_rate_first,
    decay_base_first,
    head_scale_first,
    receptance_second,
    key_second_group,
    value_second_group,
    decay_preact_second,
    context_rate_second,
    decay_base_second,
    head_scale_second,
    decay_extra_log,
    output_weight_first,
    output_weight_second,
    feedforward_gain,
    routed_expert_index,
    routed_expert_weight,
    expert_gate_weight,
    expert_up_weight,
    expert_down_weight,
    shared_gate_weight,
    shared_up_weight,
    shared_down_weight,
):
    rows = receptance_first.shape[0]
    width = residual.shape[1]
    read_a, map_a, read_b, map_b, message = local_call(
        (
            receptance_first,
            key_first_group,
            value_first_group,
            decay_preact_first,
            context_rate_first,
            decay_base_first[None, :],
            receptance_second,
            key_second_group,
            value_second_group,
            decay_preact_second,
            context_rate_second,
            decay_base_second[None, :],
            decay_extra_log.reshape(-1, SPAN),
        )
    )
    enter_a, enter_b = exchange_call(message)
    partial = project_call(
        (
            read_a,
            map_a,
            enter_a,
            head_scale_first[None, :],
            output_weight_first,
            read_b,
            map_b,
            enter_b,
            head_scale_second[None, :],
            output_weight_second,
        ),
        rows,
        width,
    )
    summed = scatter_call(partial.reshape(-1, residual.shape[0], width))
    devices = lax.axis_size(ALL)
    attended, normed, slots = dispatch_call(
        residual, summed, feedforward_gain[None, :], routed_expert_index, devices
    )
    arrived = exchange_slots(slots)
    result = expert_call(
        arrived, expert_gate_weight[0], expert_up_weight[0], expert_down_weight[0]
    )
    returned = exchange_slots(result)
    shared_out = jnp.dot(
        swiglu_hidden(normed, shared_gate_weight, shared_up_weight),
        shared_down_weight,
        preferred_element_type=F32,
    )
    return combine_call(attended, shared_out, returned, routed_expert_index, routed_expert_weight)


def solution(mesh):
    finer = Mesh(mesh.devices.reshape(4, 4, 4, 2), ALL)
    sp, tp = (Z, X), (Y, C)
    heads = (P(sp, tp),) * 5 + (P(tp),) * 2
    placed = (
        (P(ALL, None),)
        + heads
        + heads
        + (P(sp), P(tp, None), P(tp, None), P(), P(ALL, None), P(ALL, None))
        + (P(ALL, None, None),) * 3
        + (P(),) * 3
    )
    return jax.shard_map(
        local, mesh=finer, in_specs=placed, out_specs=P(ALL, None), check_vma=False
    )
```

```python
import functools
import itertools

import jax
import jax.numpy as jnp
import numpy as np
from jax import lax
from jax.experimental import pallas as pl
from jax.experimental.pallas import tpu as pltpu
from jax.sharding import Mesh
from jax.sharding import PartitionSpec as P

F32, BF16 = jnp.float32, jnp.bfloat16
SPAN = 128
LANES = 128
KEY_EPSILON = 1e-06
HEAD_EPSILON = 0.00064
NORM_EPSILON = 1e-06


def nn(a, b):
    return lax.dot_general(a, b, (((1,), (0,)), ((), ())), preferred_element_type=F32)


def nt(a, b):
    return lax.dot_general(a, b, (((1,), (1,)), ((), ())), preferred_element_type=F32)


def halves(x):
    high = x.astype(BF16)
    return high, (x - high.astype(F32)).astype(BF16)


def dot1(f, a, b):
    return f(a.astype(BF16), b.astype(BF16))


def dot3(f, a, b):
    ah, al = halves(a)
    bh, bl = halves(b)
    return f(ah, bh) + (f(ah, bl) + f(al, bh))


def iota(shape, dim):
    return lax.broadcasted_iota(jnp.int32, shape, dim)


def head_sum(x, width):
    if width == LANES:
        return jnp.sum(x, axis=-1, keepdims=True)
    lane = iota(x.shape, 1)
    left = jnp.sum(jnp.where(lane < width, x, 0.0), axis=-1, keepdims=True)
    right = jnp.sum(jnp.where(lane < width, 0.0, x), axis=-1, keepdims=True)
    return jnp.where(lane < width, left, right)


def local_kernel(dot, *refs):
    (r_a, k_a, v_a, p_a, c_a, base_a, r_b, k_b, v_b, p_b, c_b, base_b, extra_ref) = refs[:13]
    read_a, map_a, read_b, map_b, message = refs[13:]
    square = (SPAN, SPAN)
    row, col = iota(square, 0), iota(square, 1)
    lower = row >= col
    strict = row > col
    lower_bf = jnp.where(lower, 1.0, 0.0).astype(BF16)
    eye = jnp.where(row == col, 1.0, 0.0)
    count = r_a.shape[0] // SPAN
    items = []
    for group, (r_, k_, v_, p_, c_, base_, width) in enumerate(
        ((r_a, k_a, v_a, p_a, c_a, base_a, 64), (r_b, k_b, v_b, p_b, c_b, base_b, 128))
    ):
        for block in range(count):
            at = pl.ds(block * SPAN, SPAN)
            key = k_[at, :].astype(F32)
            unit = key * lax.rsqrt(head_sum(key * key, width) + KEY_EPSILON)
            removal = unit * jax.nn.sigmoid(c_[at, :].astype(F32))
            slow = jax.nn.sigmoid(p_[at, :].astype(F32))
            extra = extra_ref[pl.ds(block, 1), :]
            rate = 2.0 * base_[...]
            high, low = halves(slow)
            run_slow = nn(lower_bf, high) + nn(lower_bf, low)
            run_extra = jnp.sum(jnp.where(lower, extra, 0.0), axis=-1, keepdims=True)
            own_extra = jnp.sum(jnp.where(row == col, extra, 0.0), axis=-1, keepdims=True)
            running = run_extra - rate * run_slow
            own_log = own_extra - rate * slow
            centre = running[SPAN // 2 - 1 : SPAN // 2, :]
            ending = running[SPAN - 1 : SPAN, :]
            grown = running - centre
            read = r_[at, :].astype(F32) * jnp.exp(grown)
            query = unit * jnp.exp(grown - own_log)
            write = removal * jnp.exp(-grown)
            write_end = write * jnp.exp(ending - centre)
            items.append(
                dict(
                    group=group,
                    block=block,
                    width=width,
                    read=read,
                    query=query,
                    write=write,
                    write_end=write_end,
                    value=v_[at, :].astype(F32),
                    centre=jnp.exp(centre),
                    ending=jnp.exp(ending),
                )
            )
    solves = []
    for item in items:
        lane = col < item["width"]
        masks = [None] if item["width"] == SPAN else [lane, jnp.logical_not(lane)]
        item["parts"] = []
        for mask in masks:
            query = item["query"] if mask is None else jnp.where(mask, item["query"], 0.0)
            read = item["read"] if mask is None else jnp.where(mask, item["read"], 0.0)
            both = dot(nt, jnp.concatenate([query, read], axis=0), item["write"])
            coupling = jnp.where(strict, both[:SPAN], 0.0)
            reading = jnp.where(lower, both[SPAN:], 0.0)
            part = dict(mask=mask, coupling=coupling, reading=reading)
            item["parts"].append(part)
            solves.append(part)
    size = 1
    while size < SPAN:
        near = ((row // (2 * size)) == (col // (2 * size))) & ((row // size) > (col // size))
        for part in solves:
            step = jnp.where(near, part["coupling"], 0.0)
            if size == 1:
                part["inverse"] = eye - step
            else:
                inverse = part["inverse"]
                part["inverse"] = inverse - dot(nn, dot(nn, inverse, step), inverse)
        size *= 2
    head_row, head_col = row < 64, col < 64
    same_head = head_row == head_col
    for item in items:
        parts = item["parts"]
        right = jnp.concatenate([item["value"], -item["query"]], axis=1)
        wide = iota(right.shape, 1) % SPAN < 64

        def spread(x):
            if len(parts) == 1:
                return x
            return jnp.concatenate([jnp.where(wide, x, 0.0), jnp.where(wide, 0.0, x)], axis=0)

        def joined(name):
            return jnp.concatenate([part[name] for part in parts], axis=1)

        solved = dot(nn, joined("inverse"), spread(right))
        given = dot(nn, joined("reading"), spread(solved))
        item["local_read"] = given[:, :SPAN]
        item["state_read"] = (item["read"] + given[:, SPAN:]) * item["centre"]
        scaled = jnp.concatenate([solved[:, :SPAN], solved[:, SPAN:] * item["centre"]], axis=1)
        step = dot(nn, item["write_end"].T, scaled)
        diagonal = jnp.where(row == col, item["ending"], 0.0)
        step = step + jnp.concatenate([jnp.zeros(square, F32), diagonal], axis=1)
        if item["width"] < SPAN:
            both_heads = jnp.concatenate([same_head, same_head], axis=1)
            step = jnp.where(both_heads, step, 0.0)
        item["step"] = step
    for group, (read_ref, map_ref) in enumerate(((read_a, map_a), (read_b, map_b))):
        held = None
        for item in items:
            if item["group"] != group:
                continue
            at = pl.ds(item["block"] * SPAN, SPAN)
            if held is None:
                read_ref[at, :] = item["local_read"]
                map_ref[at, :] = item["state_read"].astype(BF16)
                held = item["step"]
            else:
                out = dot(nn, item["state_read"], held)
                read_ref[at, :] = item["local_read"] + out[:, :SPAN]
                map_ref[at, :] = out[:, SPAN:].astype(BF16)
                step = item["step"]
                held = dot(nn, step[:, SPAN:], held)
                held = jnp.concatenate([held[:, :SPAN] + step[:, :SPAN], held[:, SPAN:]], axis=1)
        if group == 0:
            message[0:64, :] = (held[:64, :] + held[64:, :]).astype(BF16)
        else:
            message[64:192, :] = held.astype(BF16)


def local_call(args, dot=dot1):
    rows = args[0].shape[0]
    shapes = [
        jax.ShapeDtypeStruct((rows, LANES), F32),
        jax.ShapeDtypeStruct((rows, LANES), BF16),
        jax.ShapeDtypeStruct((rows, LANES), F32),
        jax.ShapeDtypeStruct((rows, LANES), BF16),
        jax.ShapeDtypeStruct((192, 2 * LANES), BF16),
    ]
    return pl.pallas_call(
        functools.partial(local_kernel, dot),
        out_shape=shapes,
        in_specs=[pl.BlockSpec(memory_space=pltpu.VMEM)] * 13,
        out_specs=[pl.BlockSpec(memory_space=pltpu.VMEM)] * 5,
        name="local_terms",
    )(*args)


Z, X, Y, C = "z", "x", "y", "core"
ALL = (Z, X, Y, C)
MESH = pl.DeviceIdType.MESH
VMEM = pltpu.VMEM


def whole(count):
    return [pl.BlockSpec(memory_space=pltpu.VMEM)] * count


def greet(peers):
    barrier = pltpu.get_barrier_semaphore()
    for peer in peers:
        pl.semaphore_signal(barrier, inc=1, device_id=peer, device_id_type=MESH)
    pl.semaphore_wait(barrier, len(peers))


def follow(step, held):
    high, low = halves(held)
    moved = nn(step[:, LANES:], high) + nn(step[:, LANES:], low)
    return moved


def exchange_kernel(
    message, enter_a, enter_b, rows, columns, total, row_send, row_recv, col_send, col_recv
):
    z, x, y, c = [lax.axis_index(name) for name in ALL]
    row_peers = [(z, lax.rem(x + d, 4), y, c) for d in range(1, 4)]
    col_peers = [(lax.rem(z + d, 4), x, y, c) for d in range(1, 4)]
    greet(row_peers + col_peers)

    def row_copy(d):
        return pltpu.make_async_remote_copy(
            src_ref=message,
            dst_ref=rows.at[d],
            send_sem=row_send.at[d],
            recv_sem=row_recv.at[d],
            device_id=row_peers[d - 1],
            device_id_type=MESH,
        )

    def col_copy(d):
        return pltpu.make_async_remote_copy(
            src_ref=total,
            dst_ref=columns.at[d],
            send_sem=col_send.at[d],
            recv_sem=col_recv.at[d],
            device_id=col_peers[d - 1],
            device_id_type=MESH,
        )

    for d in (2, 1, 3):
        row_copy(d).start()
    rows[0] = message[...]
    square = (LANES, 2 * LANES)
    row, col = iota(square, 0), iota(square, 1)
    same = (row < 64) == (col % LANES < 64)
    unit = jnp.where(row + LANES == col, 1.0, 0.0)
    for d in range(1, 4):
        row_copy(d).wait()

    def steps(packed):
        top = packed[0:64, :]
        first = jnp.where(same, jnp.concatenate([top, top], axis=0), jnp.zeros((), BF16))
        return first, packed[64:192, :]

    def chain(step, held):
        moved = follow(step, held)
        own = step[:, :LANES].astype(F32)
        return jnp.concatenate([moved[:, :LANES] + own, moved[:, LANES:]], axis=1)

    inside = [unit, unit]
    running = [unit, unit]
    for k in range(4):
        pair = steps(rows[lax.rem(x - k + 4, 4)])
        inside = [jnp.where(x == k, now, old) for now, old in zip(running, inside)]
        if k == 0:
            running = [p.astype(F32) for p in pair]
        else:
            running = [chain(p, r) for p, r in zip(pair, running)]
    total[0:64, :] = (running[0][:64, :] + running[0][64:, :]).astype(BF16)
    total[64:192, :] = running[1].astype(BF16)
    for d in (2, 1, 3):

        @pl.when(z + d < 4)
        def _():
            col_copy(d).start()

    enter_a[...] = jnp.zeros_like(enter_a)
    enter_b[...] = jnp.zeros_like(enter_b)
    for k in range(3):

        @pl.when(k < z)
        def _():
            d = z - k
            pltpu.make_async_remote_copy(
                src_ref=total,
                dst_ref=columns.at[d],
                send_sem=col_send.at[d],
                recv_sem=col_recv.at[d],
                device_id=(k, x, y, c),
                device_id_type=MESH,
            ).wait_recv()
            pair = steps(columns[d])
            for enter, step in zip((enter_a, enter_b), pair):
                enter[...] = follow(step, enter[...]) + step[:, :LANES].astype(F32)

    for enter, own in zip((enter_a, enter_b), inside):
        enter[...] = dot3(nn, own[:, LANES:], enter[...]) + own[:, :LANES]
    for d in (2, 1, 3):

        @pl.when(z + d < 4)
        def _():
            col_copy(d).wait_send()


def exchange_call(message):
    shape = jax.ShapeDtypeStruct((LANES, LANES), F32)
    return pl.pallas_call(
        exchange_kernel,
        out_shape=[shape, shape],
        in_specs=whole(1),
        out_specs=whole(2),
        scratch_shapes=[
            pltpu.VMEM((4, 192, 2 * LANES), BF16),
            pltpu.VMEM((4, 192, 2 * LANES), BF16),
            pltpu.VMEM((192, 2 * LANES), BF16),
        ]
        + [pltpu.SemaphoreType.DMA((4,))] * 4,
        compiler_params=pltpu.CompilerParams(collective_id=1, has_side_effects=True),
        name="exchange",
    )(message)


def project_kernel(
    read_a, map_a, enter_a, gain_a, weight_a, read_b, map_b, enter_b, gain_b, weight_b, out
):
    square = (LANES, LANES)
    row, col = iota(square, 0), iota(square, 1)
    mixed = []
    for read, map_, enter, gain, width in (
        (read_a, map_a, enter_a, gain_a, 64),
        (read_b, map_b, enter_b, gain_b, 128),
    ):
        mean = jnp.where((row // width) == (col // width), 1.0 / width, 0.0).astype(BF16)
        high, low = halves(enter[...])
        readout = read[...] + nn(map_[...], high) + nn(map_[...], low)
        high, low = halves(readout)
        centred = readout - (nn(high, mean) + nn(low, mean))
        high, low = halves(centred * centred)
        spread = nn(high, mean) + nn(low, mean)
        mixed.append((centred * lax.rsqrt(spread + HEAD_EPSILON) * gain[...]).astype(BF16))
    rows, width = out.shape
    both = jnp.concatenate(mixed, axis=1)
    weight = jnp.concatenate([weight_a[...], weight_b[...]], axis=0)
    for at in range(0, width, 512):
        out[:, at : at + 512] = nn(both, weight[:, at : at + 512]).astype(BF16)


def project_call(args, rows, width):
    return pl.pallas_call(
        project_kernel,
        out_shape=jax.ShapeDtypeStruct((rows, width), BF16),
        in_specs=whole(10),
        out_specs=whole(1)[0],
        name="project",
    )(*args)


def scatter_kernel(part, out, pair_in, own, ring_in, pair_send, pair_recv, ring_send, ring_recv):
    z, x, y, c = [lax.axis_index(name) for name in ALL]
    partner = (z, x, y, 1 - c)
    peers = [(z, x, lax.rem(y + d, 4), c) for d in range(1, 4)]
    greet([partner] + peers)
    rows = out.shape[0]

    def pair_copy(d):
        goal = lax.rem(y + d, 4)
        return pltpu.make_async_remote_copy(
            src_ref=part.at[goal * 2 + (1 - c)],
            dst_ref=pair_in.at[d],
            send_sem=pair_send.at[d],
            recv_sem=pair_recv.at[d],
            device_id=partner,
            device_id_type=MESH,
        )

    def ring_copy(d):
        return pltpu.make_async_remote_copy(
            src_ref=own.at[d],
            dst_ref=ring_in.at[d],
            send_sem=ring_send.at[d],
            recv_sem=ring_recv.at[d],
            device_id=peers[d - 1],
            device_id_type=MESH,
        )

    for d in (2, 1, 3, 0):
        pair_copy(d).start()
    for d in (2, 1, 3):
        pair_copy(d).wait()
        goal = lax.rem(y + d, 4)
        own[d] = (part[goal * 2 + c].astype(F32) + pair_in[d].astype(F32)).astype(BF16)
        ring_copy(d).start()
    pair_copy(0).wait()
    out[...] = part[y * 2 + c].astype(F32) + pair_in[0].astype(F32)
    for d in (1, 3, 2):
        ring_copy(d).wait()
        out[...] += ring_in[d].astype(F32)


def scatter_call(part):
    blocks, rows, width = part.shape
    return pl.pallas_call(
        scatter_kernel,
        out_shape=jax.ShapeDtypeStruct((rows, width), F32),
        in_specs=whole(1),
        out_specs=whole(1)[0],
        scratch_shapes=[pltpu.VMEM((4, rows, width), BF16)] * 3
        + [pltpu.SemaphoreType.DMA((4,))] * 4,
        compiler_params=pltpu.CompilerParams(collective_id=2, has_side_effects=True),
        name="scatter_sum",
    )(part)


SLOTS = 4
PARTS = 4
UNIT = SLOTS * PARTS


DISTANCE = lambda move: sum(min(step, 4 - step) for step in move[:3])
MOVES = sorted(
    itertools.product(range(4), range(4), range(4), range(2)),
    key=lambda move: (-DISTANCE(move), -move[3]),
)
GROUP = 256
CHUNKS = 4


def shift(position, move, sign):
    moved = []
    for at, step, size in zip(position, move, (4, 4, 4, 2)):
        step = step if sign > 0 else (size - step) % size
        moved.append(lax.rem(at + step, size) if step else at)
    return tuple(moved)


def moe_kernel(
    residual,
    summed,
    gain,
    index,
    weights,
    slot_of,
    gate,
    up,
    down,
    shared_gate,
    shared_up,
    shared_down,
    out,
    sent,
    arrived,
    back,
    returned,
    gate_v,
    up_v,
    down_v,
    shared_gate_v,
    shared_up_v,
    shared_down_v,
    rows_,
    hidden,
    match_high,
    match_low,
    base,
    load_sem,
    out_send,
    out_recv,
    back_send,
    back_recv,
):
    z, x, y, c = position = tuple(lax.axis_index(name) for name in ALL)
    devices = len(MOVES)
    loads = [
        pltpu.make_async_copy(a, b, load_sem.at[k])
        for k, (a, b) in enumerate(
            (
                (shared_gate, shared_gate_v),
                (shared_up, shared_up_v),
                (shared_down, shared_down_v),
                (gate, gate_v),
                (up, up_v),
                (down, down_v),
            )
        )
    ]
    for load in loads:
        load.start()

    def unit(k):
        return pl.ds(k * UNIT, UNIT)

    def out_copy(k):
        return pltpu.make_async_remote_copy(
            src_ref=sent.at[unit(k)],
            dst_ref=arrived.at[unit(k)],
            send_sem=out_send.at[k],
            recv_sem=out_recv.at[k],
            device_id=shift(position, MOVES[k], 1),
            device_id_type=MESH,
        )

    def back_copy(k):
        return pltpu.make_async_remote_copy(
            src_ref=back.at[unit(k)],
            dst_ref=returned.at[unit(k)],
            send_sem=back_send.at[k],
            recv_sem=back_recv.at[k],
            device_id=shift(position, MOVES[k], -1),
            device_id_type=MESH,
        )

    total = (residual[...].astype(F32) + summed[...]).astype(BF16)
    wide = total.astype(F32)
    mean = jnp.mean(wide * wide, axis=-1, keepdims=True)
    normed = (wide * lax.rsqrt(mean + NORM_EPSILON) * gain[...]).astype(BF16)
    base[...] = wide
    rows, width = normed.shape
    part = width // PARTS
    stacked = jnp.concatenate([normed[:, q * part : (q + 1) * part] for q in range(PARTS)], axis=0)

    ids = index[...]
    relative = (
        ((((ids >> 5) - z) & 3) << 5)
        + ((((ids >> 3) - x) & 3) << 3)
        + ((((ids >> 1) - y) & 3) << 1)
        + ((ids - c) & 1)
    )
    lanes = iota((rows, LANES), 1)
    chosen = jnp.zeros((rows, LANES), F32)
    scale = jnp.zeros((rows, LANES), F32)
    for k in range(ids.shape[1]):
        here = relative[:, k : k + 1] == lanes
        chosen += jnp.where(here, 1.0, 0.0)
        scale += jnp.where(here, weights[:, k : k + 1], 0.0)
    chosen = nn(chosen.astype(BF16), slot_of[...])
    high, low = [nn(half, slot_of[...]).astype(BF16) for half in halves(scale)]
    earlier = jnp.where(iota((rows, rows), 0) > iota((rows, rows), 1), 1.0, 0.0).astype(BF16)
    rank = nn(earlier, chosen.astype(BF16))
    code = jnp.concatenate([(chosen * (rank + 1.0)).astype(BF16)] * PARTS, axis=0)
    high, low = [jnp.concatenate([half] * PARTS, axis=0) for half in (high, low)]

    groups = sent.shape[0] // GROUP
    per = GROUP // UNIT
    shape = (GROUP, PARTS * rows)
    place = iota(shape, 0) % UNIT
    fits = (place // SLOTS) == (iota(shape, 1) // rows)
    wanted = (place % SLOTS + 1).astype(F32)

    def select(k):
        found = (iota((GROUP, LANES), 0) + GROUP * k) // UNIT == iota((GROUP, LANES), 1)
        return jnp.where(found, 1.0, 0.0).astype(BF16)

    def launch(k):
        for slot in range(per * k, min(per * (k + 1), devices - 1)):
            out_copy(slot).start()

    for k in range(groups):
        found = nt(select(k), code)
        taken = jnp.where(fits & (found == wanted), 1.0, 0.0).astype(BF16)
        sent[GROUP * k : GROUP * (k + 1), :] = nn(taken, stacked).astype(BF16)
        if k:
            launch(k - 1)
    launch(groups - 1)
    arrived[unit(devices - 1), :] = sent[unit(devices - 1), :]

    for load in loads[:2]:
        load.wait()
    gate_val = nn(normed, shared_gate_v[...])
    up_val = nn(normed, shared_up_v[...])
    shared = (gate_val * jax.nn.sigmoid(gate_val) * up_val).astype(BF16)
    loads[2].wait()
    for at in range(0, width, 512):
        base[:, at : at + 512] += nn(shared, shared_down_v[:, at : at + 512])

    shape = (PARTS * rows, GROUP)
    place = iota(shape, 1) % UNIT
    fits = (place // SLOTS) == (iota(shape, 0) // rows)
    wanted = (place % SLOTS + 1).astype(F32)
    for k in range(groups):
        chosen_here = select(k)
        match = fits & (nt(code, chosen_here) == wanted)
        match_high[k] = jnp.where(match, nt(high, chosen_here), 0.0).astype(BF16)
        match_low[k] = jnp.where(match, nt(low, chosen_here), 0.0).astype(BF16)

    a, b = iota((GROUP, GROUP), 0), iota((GROUP, GROUP), 1)
    here = (b % UNIT // SLOTS) * 64 + (b // UNIT) * SLOTS + b % SLOTS
    order = jnp.where(a == here, 1.0, 0.0).astype(BF16)
    there = (a % UNIT // SLOTS) * 64 + (a // UNIT) * SLOTS + a % SLOTS
    order_back = jnp.where(b == there, 1.0, 0.0).astype(BF16)
    for load in loads[3:]:
        load.wait()

    span = groups // CHUNKS

    def reply(k):
        for slot in range(per * span * k, min(per * span * (k + 1), devices - 1)):
            back_copy(slot).start()

    for chunk in range(CHUNKS):
        for slot in range(per * span * chunk, min(per * span * (chunk + 1), devices - 1)):
            out_copy(slot).wait_recv()
        for g in range(span):
            k = chunk * span + g
            sorted_ = nn(order, arrived[GROUP * k : GROUP * (k + 1), :]).astype(BF16)
            for q in range(PARTS):
                rows_[64 * g : 64 * (g + 1), q * part : (q + 1) * part] = sorted_[
                    64 * q : 64 * (q + 1)
                ]
        for at in range(0, hidden.shape[1], 256):
            gate_val = nn(rows_[...], gate_v[:, at : at + 256])
            up_val = nn(rows_[...], up_v[:, at : at + 256])
            hidden[:, at : at + 256] = (gate_val * jax.nn.sigmoid(gate_val) * up_val).astype(BF16)
        for at in range(0, width, 512):
            rows_[:, at : at + 512] = nn(hidden[...], down_v[:, at : at + 512]).astype(BF16)
        for g in range(span):
            k = chunk * span + g
            gathered = jnp.concatenate(
                [rows_[64 * g : 64 * (g + 1), q * part : (q + 1) * part] for q in range(PARTS)],
                axis=0,
            )
            back[GROUP * k : GROUP * (k + 1), :] = nn(order_back, gathered).astype(BF16)
        reply(chunk)
    returned[unit(devices - 1), :] = back[unit(devices - 1), :]

    routed = jnp.zeros((PARTS * rows, part), F32)
    for k in range(groups):
        for slot in range(per * k, min(per * (k + 1), devices - 1)):
            back_copy(slot).wait_recv()
        block = returned[GROUP * k : GROUP * (k + 1), :]
        routed += nn(match_high[k], block) + nn(match_low[k], block)
    for q in range(PARTS):
        at = slice(q * part, (q + 1) * part)
        out[:, at] = (base[:, at] + routed[q * rows : (q + 1) * rows, :]).astype(BF16)
    for slot in range(devices - 1):
        out_copy(slot).wait_send()
        back_copy(slot).wait_send()


def moe_call(residual, summed, gain, index, weights, gate, up, down, *shared):
    rows, width = residual.shape
    devices = len(MOVES)
    slot_of = np.zeros((devices, devices), np.float32)
    for slot, (dz, dx, dy, dc) in enumerate(MOVES):
        slot_of[((dz * 4 + dx) * 4 + dy) * 2 + dc, slot] = 1.0
    slots = pltpu.VMEM((devices * UNIT, width // PARTS), BF16)
    groups = devices * UNIT // GROUP
    match = pltpu.VMEM((groups, PARTS * rows, GROUP), BF16)
    chunk_rows = devices * SLOTS // CHUNKS
    return pl.pallas_call(
        moe_kernel,
        out_shape=jax.ShapeDtypeStruct((rows, width), BF16),
        in_specs=whole(6) + [pl.BlockSpec(memory_space=pl.ANY)] * 6,
        out_specs=whole(1)[0],
        scratch_shapes=[slots] * 4
        + [pltpu.VMEM(a.shape, BF16) for a in (gate, up, down, *shared)]
        + [
            pltpu.VMEM((chunk_rows, width), BF16),
            pltpu.VMEM((chunk_rows, gate.shape[1]), BF16),
            match,
            match,
            pltpu.VMEM((rows, width), F32),
            pltpu.SemaphoreType.DMA((6,)),
        ]
        + [pltpu.SemaphoreType.DMA((devices,))] * 4,
        compiler_params=pltpu.CompilerParams(
            has_side_effects=True, vmem_limit_bytes=48 * 1024 * 1024
        ),
        name="experts",
    )(residual, summed, gain, index, weights, jnp.asarray(slot_of, BF16), gate, up, down, *shared)


def local(
    residual,
    receptance_first,
    key_first_group,
    value_first_group,
    decay_preact_first,
    context_rate_first,
    decay_base_first,
    head_scale_first,
    receptance_second,
    key_second_group,
    value_second_group,
    decay_preact_second,
    context_rate_second,
    decay_base_second,
    head_scale_second,
    decay_extra_log,
    output_weight_first,
    output_weight_second,
    feedforward_gain,
    routed_expert_index,
    routed_expert_weight,
    expert_gate_weight,
    expert_up_weight,
    expert_down_weight,
    shared_gate_weight,
    shared_up_weight,
    shared_down_weight,
):
    rows = receptance_first.shape[0]
    width = residual.shape[1]
    read_a, map_a, read_b, map_b, message = local_call(
        (
            receptance_first,
            key_first_group,
            value_first_group,
            decay_preact_first,
            context_rate_first,
            decay_base_first[None, :],
            receptance_second,
            key_second_group,
            value_second_group,
            decay_preact_second,
            context_rate_second,
            decay_base_second[None, :],
            decay_extra_log.reshape(-1, SPAN),
        )
    )
    enter_a, enter_b = exchange_call(message)
    partial = project_call(
        (
            read_a,
            map_a,
            enter_a,
            head_scale_first[None, :],
            output_weight_first,
            read_b,
            map_b,
            enter_b,
            head_scale_second[None, :],
            output_weight_second,
        ),
        rows,
        width,
    )
    summed = scatter_call(partial.reshape(-1, residual.shape[0], width))
    return moe_call(
        residual,
        summed,
        feedforward_gain[None, :],
        routed_expert_index,
        routed_expert_weight,
        expert_gate_weight[0],
        expert_up_weight[0],
        expert_down_weight[0],
        shared_gate_weight,
        shared_up_weight,
        shared_down_weight,
    )


def solution(mesh):
    finer = Mesh(mesh.devices.reshape(4, 4, 4, 2), ALL)
    sp, tp = (Z, X), (Y, C)
    heads = (P(sp, tp),) * 5 + (P(tp),) * 2
    placed = (
        (P(ALL, None),)
        + heads
        + heads
        + (P(sp), P(tp, None), P(tp, None), P(), P(ALL, None), P(ALL, None))
        + (P(ALL, None, None),) * 3
        + (P(),) * 3
    )
    return jax.shard_map(
        local, mesh=finer, in_specs=placed, out_specs=P(ALL, None), check_vma=False
    )
```

```python
import functools
import itertools

import jax
import jax.numpy as jnp
import numpy as np
from jax import lax
from jax.experimental import pallas as pl
from jax.experimental.pallas import tpu as pltpu
from jax.sharding import Mesh
from jax.sharding import PartitionSpec as P

F32, BF16 = jnp.float32, jnp.bfloat16
SPAN = 128
LANES = 128
HEAD_SIZE_FIRST = 64
KEY_EPSILON = 1e-06
HEAD_EPSILON = 0.00064
NORM_EPSILON = 1e-06
Z, X, Y, C = "z", "x", "y", "core"
ALL = (Z, X, Y, C)
MESH = pl.DeviceIdType.MESH
SLOTS = 4
PARTS = 4
UNIT = SLOTS * PARTS
GROUP = 256
CHUNKS = 4


def distance(move):
    return sum(min(step, 4 - step) for step in move[:3])


MOVES = sorted(
    itertools.product(range(4), range(4), range(4), range(2)),
    key=lambda move: (-distance(move), -move[3]),
)


def nn(a, b):
    return lax.dot_general(a, b, (((1,), (0,)), ((), ())), preferred_element_type=F32)


def nt(a, b):
    return lax.dot_general(a, b, (((1,), (1,)), ((), ())), preferred_element_type=F32)


def halves(x):
    high = x.astype(BF16)
    return high, (x - high.astype(F32)).astype(BF16)


def dot(f, a, b):
    return f(a.astype(BF16), b.astype(BF16))


def dot3(f, a, b):
    ah, al = halves(a)
    bh, bl = halves(b)
    return f(ah, bh) + (f(ah, bl) + f(al, bh))


def iota(shape, dim):
    return lax.broadcasted_iota(jnp.int32, shape, dim)


def head_sum(x, width):
    if width == LANES:
        return jnp.sum(x, axis=-1, keepdims=True)
    lane = iota(x.shape, 1)
    left = jnp.sum(jnp.where(lane < width, x, 0.0), axis=-1, keepdims=True)
    right = jnp.sum(jnp.where(lane < width, 0.0, x), axis=-1, keepdims=True)
    return jnp.where(lane < width, left, right)


def shift(position, move, sign):
    moved = []
    for at, step, size in zip(position, move, (4, 4, 4, 2)):
        step = step if sign > 0 else (size - step) % size
        moved.append(lax.rem(at + step, size) if step else at)
    return tuple(moved)


def block_terms(groups, extra_ref):
    square = (SPAN, SPAN)
    row, col = iota(square, 0), iota(square, 1)
    lower = row >= col
    lower_bf = jnp.where(lower, 1.0, 0.0).astype(BF16)
    items = []
    for group, (r_, k_, v_, p_, c_, base_, width) in enumerate(groups):
        for block in range(r_.shape[0] // SPAN):
            at = pl.ds(block * SPAN, SPAN)
            key = k_[at, :].astype(F32)
            unit = key * lax.rsqrt(head_sum(key * key, width) + KEY_EPSILON)
            removal = unit * jax.nn.sigmoid(c_[at, :].astype(F32))
            slow = jax.nn.sigmoid(p_[at, :].astype(F32))
            extra = extra_ref[pl.ds(block, 1), :]
            rate = 2.0 * base_[...]
            high, low = halves(slow)
            run_slow = nn(lower_bf, high) + nn(lower_bf, low)
            run_extra = jnp.sum(jnp.where(lower, extra, 0.0), axis=-1, keepdims=True)
            own_extra = jnp.sum(jnp.where(row == col, extra, 0.0), axis=-1, keepdims=True)
            running = run_extra - rate * run_slow
            own_log = own_extra - rate * slow
            centre = running[SPAN // 2 - 1 : SPAN // 2, :]
            ending = running[SPAN - 1 : SPAN, :]
            grown = running - centre
            write = removal * jnp.exp(-grown)
            items.append(
                dict(
                    group=group,
                    block=block,
                    width=width,
                    read=r_[at, :].astype(F32) * jnp.exp(grown),
                    query=unit * jnp.exp(grown - own_log),
                    write=write,
                    write_end=write * jnp.exp(ending - centre),
                    value=v_[at, :].astype(F32),
                    centre=jnp.exp(centre),
                    ending=jnp.exp(ending),
                )
            )
    return items


def spread(item, x):
    if len(item["parts"]) == 1:
        return x
    first = iota(x.shape, 1) % SPAN < HEAD_SIZE_FIRST
    return jnp.concatenate([jnp.where(first, x, 0.0), jnp.where(first, 0.0, x)], axis=0)


def joined(item, name):
    return jnp.concatenate([part[name] for part in item["parts"]], axis=1)


def block_steps(items):
    square = (SPAN, SPAN)
    row, col = iota(square, 0), iota(square, 1)
    strict = row > col
    lower = row >= col
    eye = jnp.where(row == col, 1.0, 0.0)
    solves = []
    for item in items:
        lane = col < item["width"]
        masks = [None] if item["width"] == SPAN else [lane, jnp.logical_not(lane)]
        item["parts"] = []
        for mask in masks:
            query = item["query"] if mask is None else jnp.where(mask, item["query"], 0.0)
            read = item["read"] if mask is None else jnp.where(mask, item["read"], 0.0)
            both = dot(nt, jnp.concatenate([query, read], axis=0), item["write"])
            part = dict(
                coupling=jnp.where(strict, both[:SPAN], 0.0),
                reading=jnp.where(lower, both[SPAN:], 0.0),
            )
            item["parts"].append(part)
            solves.append(part)
    size = 1
    while size < SPAN:
        near = ((row // (2 * size)) == (col // (2 * size))) & ((row // size) > (col // size))
        for part in solves:
            step = jnp.where(near, part["coupling"], 0.0)
            if size == 1:
                part["inverse"] = eye - step
            else:
                inverse = part["inverse"]
                part["inverse"] = inverse - dot(nn, dot(nn, inverse, step), inverse)
        size *= 2
    same_head = (row < HEAD_SIZE_FIRST) == (col < HEAD_SIZE_FIRST)
    for item in items:
        right = jnp.concatenate([item["value"], -item["query"]], axis=1)
        solved = dot(nn, joined(item, "inverse"), spread(item, right))
        item["solved"] = solved
        scaled = jnp.concatenate([solved[:, :SPAN], solved[:, SPAN:] * item["centre"]], axis=1)
        step = dot(nn, item["write_end"].T, scaled)
        diagonal = jnp.where(row == col, item["ending"], 0.0)
        step = step + jnp.concatenate([jnp.zeros(square, F32), diagonal], axis=1)
        if item["width"] < SPAN:
            step = jnp.where(jnp.concatenate([same_head, same_head], axis=1), step, 0.0)
        item["step"] = step


def block_chain(items):
    held = None
    for item in items:
        item["held"] = held
        step = item["step"]
        if held is None:
            held = step
        else:
            held = dot(nn, step[:, SPAN:], held)
            held = jnp.concatenate([held[:, :SPAN] + step[:, :SPAN], held[:, SPAN:]], axis=1)
    return held


def block_reads(items, read_ref, map_ref):
    for item in items:
        given = dot(nn, joined(item, "reading"), spread(item, item["solved"]))
        local_read = given[:, :SPAN]
        state_read = (item["read"] + given[:, SPAN:]) * item["centre"]
        at = pl.ds(item["block"] * SPAN, SPAN)
        if item["held"] is not None:
            out = dot(nn, state_read, item["held"])
            local_read = local_read + out[:, :SPAN]
            state_read = out[:, SPAN:]
        read_ref[item["group"], at, :] = local_read
        map_ref[item["group"], at, :] = state_read.astype(BF16)


def pack(ref, first, second):
    ref[0:64, :] = (first[:64, :] + first[64:, :]).astype(BF16)
    ref[64:192, :] = second.astype(BF16)


def unpack(packed):
    square = (LANES, 2 * LANES)
    same = (iota(square, 0) < 64) == (iota(square, 1) % LANES < 64)
    top = packed[0:64, :]
    first = jnp.where(same, jnp.concatenate([top, top], axis=0), jnp.zeros((), BF16))
    return first, packed[64:192, :]


def follow(step, held):
    high, low = halves(held)
    return nn(step[:, LANES:], high) + nn(step[:, LANES:], low)


def compose(step, held):
    moved = follow(step, held)
    return jnp.concatenate(
        [moved[:, :LANES] + step[:, :LANES].astype(F32), moved[:, LANES:]], axis=1
    )


def layer_kernel(
    r_a,
    k_a,
    v_a,
    p_a,
    c_a,
    base_a,
    gain_a,
    r_b,
    k_b,
    v_b,
    p_b,
    c_b,
    base_b,
    gain_b,
    extra,
    gain,
    index,
    weights,
    slot_of,
    residual,
    weight_a,
    weight_b,
    gate,
    up,
    down,
    shared_gate,
    shared_up,
    shared_down,
    out,
    residual_v,
    weight_v,
    gate_v,
    up_v,
    down_v,
    shared_gate_v,
    shared_up_v,
    shared_down_v,
    read_v,
    map_v,
    rows_v,
    columns_v,
    message,
    total,
    enter_v,
    own,
    pair_out,
    pair_in,
    ring_out,
    ring_in,
    base,
    sent,
    arrived,
    back,
    returned,
    chunk_v,
    hidden,
    match_high,
    match_low,
    load_sem,
    row_send,
    row_recv,
    col_send,
    col_recv,
    pair_send,
    pair_recv,
    ring_send,
    ring_recv,
    out_send,
    out_recv,
    back_send,
    back_recv,
):
    z, x, y, c = position = tuple(lax.axis_index(name) for name in ALL)
    devices = len(MOVES)
    barrier = pltpu.get_barrier_semaphore()
    for move in MOVES[:-1]:
        pl.semaphore_signal(
            barrier, inc=1, device_id=shift(position, move, 1), device_id_type=MESH
        )
    pairs = (
        (weight_a, weight_v.at[pl.ds(0, LANES)]),
        (weight_b, weight_v.at[pl.ds(LANES, LANES)]),
        (residual, residual_v),
        (shared_gate, shared_gate_v),
        (shared_up, shared_up_v),
        (shared_down, shared_down_v),
        (gate, gate_v),
        (up, up_v),
        (down, down_v),
    )
    loads = [pltpu.make_async_copy(a, b, load_sem.at[k]) for k, (a, b) in enumerate(pairs)]
    for load in loads:
        load.start()

    def remote(src, dst, send, recv, goal):
        return pltpu.make_async_remote_copy(
            src_ref=src,
            dst_ref=dst,
            send_sem=send,
            recv_sem=recv,
            device_id=goal,
            device_id_type=MESH,
        )

    items = block_terms(
        (
            (r_a, k_a, v_a, p_a, c_a, base_a, HEAD_SIZE_FIRST),
            (r_b, k_b, v_b, p_b, c_b, base_b, SPAN),
        ),
        extra,
    )
    block_steps(items)
    chains = [[item for item in items if item["group"] == group] for group in range(2)]
    pack(message, *[block_chain(chain) for chain in chains])
    pl.semaphore_wait(barrier, devices - 1)

    def row_copy(d):
        goal = (z, lax.rem(x + d, 4), y, c)
        return remote(message, rows_v.at[d], row_send.at[d], row_recv.at[d], goal)

    def col_copy(d):
        goal = (lax.rem(z + d, 4), x, y, c)
        return remote(total, columns_v.at[d], col_send.at[d], col_recv.at[d], goal)

    for d in (2, 1, 3):
        row_copy(d).start()
    rows_v[0] = message[...]
    for chain in chains:
        block_reads(chain, read_v, map_v)

    square = (LANES, 2 * LANES)
    unit_step = jnp.where(iota(square, 0) + LANES == iota(square, 1), 1.0, 0.0)
    inside = [unit_step, unit_step]
    running = [unit_step, unit_step]
    for d in range(1, 4):
        row_copy(d).wait()
    for k in range(4):
        pair = unpack(rows_v[lax.rem(x - k + 4, 4)])
        inside = [jnp.where(x == k, now, old) for now, old in zip(running, inside)]
        if k == 0:
            running = [p.astype(F32) for p in pair]
        else:
            running = [compose(p, r) for p, r in zip(pair, running)]
    pack(total, *running)
    for d in (2, 1, 3):

        @pl.when(z + d < 4)
        def _():
            col_copy(d).start()

    enter_v[...] = jnp.zeros_like(enter_v)
    for k in range(3):

        @pl.when(k < z)
        def _():
            d = z - k
            remote(
                total, columns_v.at[d], col_send.at[d], col_recv.at[d], (k, x, y, c)
            ).wait_recv()
            for group, step in enumerate(unpack(columns_v[d])):
                enter_v[group] = follow(step, enter_v[group]) + step[:, :LANES].astype(F32)

    entering = []
    for group, step in enumerate(inside):
        enter = dot3(nn, step[:, LANES:], enter_v[group]) + step[:, :LANES]
        entering.append(halves(enter))

    rows, width = out.shape
    half = width // 2
    partner = (z, x, y, 1 - c)
    right, left = (z, x, lax.rem(y + 1, 4), c), (z, x, lax.rem(y + 3, 4), c)

    def pair_copy(d):
        return remote(pair_out.at[d], pair_in.at[d], pair_send.at[d], pair_recv.at[d], partner)

    def ring_copy(k):
        return remote(
            ring_out.at[k],
            ring_in.at[k],
            ring_send.at[k],
            ring_recv.at[k],
            right if k % 2 == 0 else left,
        )

    square = (LANES, LANES)
    row, col = iota(square, 0), iota(square, 1)
    for load in loads[:2]:
        load.wait()
    for d in (2, 1, 3, 0):
        start = lax.rem(y + d, 4) * (2 * rows)
        theirs = pl.ds(pl.multiple_of(start + (1 - c) * rows, rows), rows)
        mine = pl.ds(pl.multiple_of(start + c * rows, rows), rows)
        mixed = []
        for group, (head_gain, size) in enumerate(((gain_a, HEAD_SIZE_FIRST), (gain_b, SPAN))):
            mean = jnp.where((row // size) == (col // size), 1.0 / size, 0.0).astype(BF16)
            high, low = entering[group]
            maps = jnp.concatenate([map_v[group, theirs, :], map_v[group, mine, :]], axis=0)
            reads = jnp.concatenate([read_v[group, theirs, :], read_v[group, mine, :]], axis=0)
            readout = reads + nn(maps, high) + nn(maps, low)
            high, low = halves(readout)
            centred = readout - (nn(high, mean) + nn(low, mean))
            high, low = halves(centred * centred)
            variance = nn(high, mean) + nn(low, mean)
            mixed.append((centred * lax.rsqrt(variance + HEAD_EPSILON) * head_gain[...]).astype(BF16))
        both = jnp.concatenate(mixed, axis=1)
        for at in range(0, width, 512):
            product = nn(both, weight_v[:, at : at + 512])
            pair_out[d, :, at : at + 512] = product[:rows].astype(BF16)
            own[d, :, at : at + 512] = product[rows:]
        pair_copy(d).start()

    pair_copy(2).wait()
    for k in range(2):
        at = slice(k * half, (k + 1) * half)
        ring_out[k] = (own[2, :, at] + pair_in[2, :, at].astype(F32)).astype(BF16)
    for k in range(2):
        ring_copy(k).start()
    for k, d, at, keep in (
        (2, 1, slice(half, width), slice(0, half)),
        (3, 3, slice(0, half), slice(half, width)),
    ):
        pair_copy(d).wait()
        ring_out[k] = (own[d, :, at] + pair_in[d, :, at].astype(F32)).astype(BF16)
        ring_copy(k).start()
        own[d, :, keep] += pair_in[d, :, keep].astype(F32)
    pair_copy(0).wait()
    loads[2].wait()
    base[...] = residual_v[...].astype(F32) + (own[0] + pair_in[0].astype(F32))
    for k, d, keep in ((4, 1, slice(0, half)), (5, 3, slice(half, width))):
        ring_copy(k - 4).wait()
        ring_out[k] = (own[d, :, keep] + ring_in[k - 4].astype(F32)).astype(BF16)
        ring_copy(k).start()
    for k, at in (
        (2, slice(half, width)),
        (3, slice(0, half)),
        (4, slice(0, half)),
        (5, slice(half, width)),
    ):
        ring_copy(k).wait()
        base[:, at] += ring_in[k].astype(F32)

    def unit(k):
        return pl.ds(k * UNIT, UNIT)

    def out_copy(k):
        return remote(
            sent.at[unit(k)],
            arrived.at[unit(k)],
            out_send.at[k],
            out_recv.at[k],
            shift(position, MOVES[k], 1),
        )

    def back_copy(k):
        return remote(
            back.at[unit(k)],
            returned.at[unit(k)],
            back_send.at[k],
            back_recv.at[k],
            shift(position, MOVES[k], -1),
        )

    wide = base[...].astype(BF16).astype(F32)
    mean = jnp.mean(wide * wide, axis=-1, keepdims=True)
    normed = (wide * lax.rsqrt(mean + NORM_EPSILON) * gain[...]).astype(BF16)
    base[...] = wide
    part = width // PARTS
    stacked = jnp.concatenate([normed[:, q * part : (q + 1) * part] for q in range(PARTS)], axis=0)

    ids = index[...]
    relative = (
        ((((ids >> 5) - z) & 3) << 5)
        + ((((ids >> 3) - x) & 3) << 3)
        + ((((ids >> 1) - y) & 3) << 1)
        + ((ids - c) & 1)
    )
    experts = iota((LANES, rows), 0)
    chosen = jnp.zeros((LANES, rows), F32)
    scale = jnp.zeros((LANES, rows), F32)
    for k in range(ids.shape[0]):
        here = relative[k : k + 1, :] == experts
        chosen += jnp.where(here, 1.0, 0.0)
        scale += jnp.where(here, weights[k : k + 1, :], 0.0)
    chosen = nn(chosen.T.astype(BF16), slot_of[...])
    high, low = [nn(term, slot_of[...]).astype(BF16) for term in halves(scale.T)]
    earlier = jnp.where(iota((rows, rows), 0) > iota((rows, rows), 1), 1.0, 0.0).astype(BF16)
    rank = nn(earlier, chosen.astype(BF16))
    code = jnp.concatenate([(chosen * (rank + 1.0)).astype(BF16)] * PARTS, axis=0)
    high, low = [jnp.concatenate([term] * PARTS, axis=0) for term in (high, low)]

    groups = sent.shape[0] // GROUP
    per = GROUP // UNIT
    shape = (GROUP, PARTS * rows)
    place = iota(shape, 0) % UNIT
    fits = (place // SLOTS) == (iota(shape, 1) // rows)
    wanted = (place % SLOTS + 1).astype(F32)

    def select(k):
        found = (iota((GROUP, LANES), 0) + GROUP * k) // UNIT == iota((GROUP, LANES), 1)
        return jnp.where(found, 1.0, 0.0).astype(BF16)

    def launch(k):
        for slot in range(per * k, min(per * (k + 1), devices - 1)):
            out_copy(slot).start()

    for k in range(groups):
        found = nt(select(k), code)
        taken = jnp.where(fits & (found == wanted), 1.0, 0.0).astype(BF16)
        sent[GROUP * k : GROUP * (k + 1), :] = nn(taken, stacked).astype(BF16)
        if k:
            launch(k - 1)
    launch(groups - 1)
    arrived[unit(devices - 1), :] = sent[unit(devices - 1), :]

    for load in loads[3:5]:
        load.wait()
    gate_val = nn(normed, shared_gate_v[...])
    up_val = nn(normed, shared_up_v[...])
    shared = (gate_val * jax.nn.sigmoid(gate_val) * up_val).astype(BF16)
    loads[5].wait()
    for at in range(0, width, 512):
        base[:, at : at + 512] += nn(shared, shared_down_v[:, at : at + 512])

    shape = (PARTS * rows, GROUP)
    place = iota(shape, 1) % UNIT
    fits = (place // SLOTS) == (iota(shape, 0) // rows)
    wanted = (place % SLOTS + 1).astype(F32)
    for k in range(groups):
        chosen_here = select(k)
        match = fits & (nt(code, chosen_here) == wanted)
        match_high[k] = jnp.where(match, nt(high, chosen_here), 0.0).astype(BF16)
        match_low[k] = jnp.where(match, nt(low, chosen_here), 0.0).astype(BF16)

    a, b = iota((GROUP, GROUP), 0), iota((GROUP, GROUP), 1)
    here = (b % UNIT // SLOTS) * 64 + (b // UNIT) * SLOTS + b % SLOTS
    order = jnp.where(a == here, 1.0, 0.0).astype(BF16)
    there = (a % UNIT // SLOTS) * 64 + (a // UNIT) * SLOTS + a % SLOTS
    order_back = jnp.where(b == there, 1.0, 0.0).astype(BF16)
    for load in loads[6:]:
        load.wait()

    span = groups // CHUNKS

    def chunk_slots(k):
        return range(per * span * k, min(per * span * (k + 1), devices - 1))

    for chunk in range(CHUNKS):
        for slot in chunk_slots(chunk):
            out_copy(slot).wait_recv()
        for g in range(span):
            k = chunk * span + g
            sorted_ = nn(order, arrived[GROUP * k : GROUP * (k + 1), :]).astype(BF16)
            for q in range(PARTS):
                chunk_v[64 * g : 64 * (g + 1), q * part : (q + 1) * part] = sorted_[
                    64 * q : 64 * (q + 1)
                ]
        for at in range(0, hidden.shape[1], 256):
            gate_val = nn(chunk_v[...], gate_v[:, at : at + 256])
            up_val = nn(chunk_v[...], up_v[:, at : at + 256])
            hidden[:, at : at + 256] = (gate_val * jax.nn.sigmoid(gate_val) * up_val).astype(BF16)
        for at in range(0, width, 512):
            chunk_v[:, at : at + 512] = nn(hidden[...], down_v[:, at : at + 512]).astype(BF16)
        for g in range(span):
            k = chunk * span + g
            gathered = jnp.concatenate(
                [chunk_v[64 * g : 64 * (g + 1), q * part : (q + 1) * part] for q in range(PARTS)],
                axis=0,
            )
            back[GROUP * k : GROUP * (k + 1), :] = nn(order_back, gathered).astype(BF16)
        for slot in chunk_slots(chunk):
            back_copy(slot).start()
    returned[unit(devices - 1), :] = back[unit(devices - 1), :]

    routed = jnp.zeros((PARTS * rows, part), F32)
    for k in range(groups):
        for slot in range(per * k, min(per * (k + 1), devices - 1)):
            back_copy(slot).wait_recv()
        block = returned[GROUP * k : GROUP * (k + 1), :]
        routed += nn(match_high[k], block) + nn(match_low[k], block)
    for q in range(PARTS):
        at = slice(q * part, (q + 1) * part)
        out[:, at] = (base[:, at] + routed[q * rows : (q + 1) * rows, :]).astype(BF16)
    for d in (2, 1, 3):

        @pl.when(z + d < 4)
        def _():
            col_copy(d).wait_send()

    for slot in range(devices - 1):
        out_copy(slot).wait_send()
        back_copy(slot).wait_send()


def slot_table():
    devices = len(MOVES)
    table = np.zeros((devices, devices), np.float32)
    for slot, (dz, dx, dy, dc) in enumerate(MOVES):
        table[((dz * 4 + dx) * 4 + dy) * 2 + dc, slot] = 1.0
    return jnp.asarray(table, BF16)


def layer_call(small, large):
    rows, width = large[0].shape
    long = small[0].shape[0]
    gate = large[3]
    devices = len(MOVES)
    part = width // PARTS
    slots = pltpu.VMEM((devices * UNIT, part), BF16)
    match = pltpu.VMEM((devices * UNIT // GROUP, PARTS * rows, GROUP), BF16)
    chunk_rows = devices * SLOTS // CHUNKS
    packed = (192, 2 * LANES)
    scratch = (
        [pltpu.VMEM((rows, width), BF16), pltpu.VMEM((2 * LANES, width), BF16)]
        + [pltpu.VMEM(a.shape, BF16) for a in large[3:]]
        + [
            pltpu.VMEM((2, long, LANES), F32),
            pltpu.VMEM((2, long, LANES), BF16),
            pltpu.VMEM((4, *packed), BF16),
            pltpu.VMEM((4, *packed), BF16),
            pltpu.VMEM(packed, BF16),
            pltpu.VMEM(packed, BF16),
            pltpu.VMEM((2, LANES, LANES), F32),
            pltpu.VMEM((4, rows, width), F32),
            pltpu.VMEM((4, rows, width), BF16),
            pltpu.VMEM((4, rows, width), BF16),
            pltpu.VMEM((6, rows, width // 2), BF16),
            pltpu.VMEM((6, rows, width // 2), BF16),
            pltpu.VMEM((rows, width), F32),
        ]
        + [slots] * 4
        + [
            pltpu.VMEM((chunk_rows, width), BF16),
            pltpu.VMEM((chunk_rows, gate.shape[1]), BF16),
            match,
            match,
            pltpu.SemaphoreType.DMA((9,)),
        ]
        + [pltpu.SemaphoreType.DMA((4,))] * 6
        + [pltpu.SemaphoreType.DMA((6,))] * 2
        + [pltpu.SemaphoreType.DMA((devices,))] * 4
    )
    return pl.pallas_call(
        layer_kernel,
        out_shape=jax.ShapeDtypeStruct((rows, width), BF16),
        in_specs=[pl.BlockSpec(memory_space=pltpu.VMEM)] * len(small)
        + [pl.BlockSpec(memory_space=pl.ANY)] * len(large),
        out_specs=pl.BlockSpec(memory_space=pltpu.VMEM),
        scratch_shapes=scratch,
        compiler_params=pltpu.CompilerParams(
            collective_id=0, has_side_effects=True, vmem_limit_bytes=60 * 1024 * 1024
        ),
        name="layer",
    )(*small, *large)


def local(
    residual,
    receptance_first,
    key_first_group,
    value_first_group,
    decay_preact_first,
    context_rate_first,
    decay_base_first,
    head_scale_first,
    receptance_second,
    key_second_group,
    value_second_group,
    decay_preact_second,
    context_rate_second,
    decay_base_second,
    head_scale_second,
    decay_extra_log,
    output_weight_first,
    output_weight_second,
    feedforward_gain,
    routed_expert_index,
    routed_expert_weight,
    expert_gate_weight,
    expert_up_weight,
    expert_down_weight,
    shared_gate_weight,
    shared_up_weight,
    shared_down_weight,
):
    small = (
        receptance_first,
        key_first_group,
        value_first_group,
        decay_preact_first,
        context_rate_first,
        decay_base_first[None, :],
        head_scale_first[None, :],
        receptance_second,
        key_second_group,
        value_second_group,
        decay_preact_second,
        context_rate_second,
        decay_base_second[None, :],
        head_scale_second[None, :],
        decay_extra_log.reshape(-1, SPAN),
        feedforward_gain[None, :],
        routed_expert_index.T,
        routed_expert_weight.T,
        slot_table(),
    )
    large = (
        residual,
        output_weight_first,
        output_weight_second,
        expert_gate_weight[0],
        expert_up_weight[0],
        expert_down_weight[0],
        shared_gate_weight,
        shared_up_weight,
        shared_down_weight,
    )
    return layer_call(small, large)


def solution(mesh):
    finer = Mesh(mesh.devices.reshape(4, 4, 4, 2), ALL)
    sp, tp = (Z, X), (Y, C)
    heads = (P(sp, tp),) * 5 + (P(tp),) * 2
    placed = (
        (P(ALL, None),)
        + heads
        + heads
        + (P(sp), P(tp, None), P(tp, None), P(), P(ALL, None), P(ALL, None))
        + (P(ALL, None, None),) * 3
        + (P(),) * 3
    )
    return jax.shard_map(
        local, mesh=finer, in_specs=placed, out_specs=P(ALL, None), check_vma=False
    )
```

```python
import functools
import itertools

import jax
import jax.numpy as jnp
import numpy as np
from jax import lax
from jax.experimental import pallas as pl
from jax.experimental.pallas import tpu as pltpu
from jax.sharding import Mesh
from jax.sharding import PartitionSpec as P

F32, BF16 = jnp.float32, jnp.bfloat16
SPAN = 128
LANES = 128
HEAD_SIZE_FIRST = 64
KEY_EPSILON = 1e-06
HEAD_EPSILON = 0.00064
NORM_EPSILON = 1e-06
Z, X, Y, C = "z", "x", "y", "core"
ALL = (Z, X, Y, C)
MESH = pl.DeviceIdType.MESH
SLOTS = 4
PARTS = 4
UNIT = SLOTS * PARTS
GROUP = 256
CHUNKS = 4
WINDOW = 4


def distance(move):
    return sum(min(step, 4 - step) for step in move[:3])


MOVES = sorted(itertools.product(range(4), range(4), range(4), range(2)), key=lambda move: (not any(move), (move[0]*32+move[1]*8+move[2]*2+move[3])*37%128))


LINES = [move for move in MOVES if sum(step > 0 for step in move) == 1]


def nn(a, b):
    return lax.dot_general(a, b, (((1,), (0,)), ((), ())), preferred_element_type=F32)


def nt(a, b):
    return lax.dot_general(a, b, (((1,), (1,)), ((), ())), preferred_element_type=F32)


def halves(x):
    high = x.astype(BF16)
    return high, (x - high.astype(F32)).astype(BF16)


def dot(f, a, b):
    return f(a.astype(BF16), b.astype(BF16))


def dot3(f, a, b):
    ah, al = halves(a)
    bh, bl = halves(b)
    return f(ah, bh) + (f(ah, bl) + f(al, bh))


def iota(shape, dim):
    return lax.broadcasted_iota(jnp.int32, shape, dim)


def head_sum(x, width):
    if width == LANES:
        return jnp.sum(x, axis=-1, keepdims=True)
    lane = iota(x.shape, 1)
    left = jnp.sum(jnp.where(lane < width, x, 0.0), axis=-1, keepdims=True)
    right = jnp.sum(jnp.where(lane < width, 0.0, x), axis=-1, keepdims=True)
    return jnp.where(lane < width, left, right)


def shift(position, move, sign):
    moved = []
    for at, step, size in zip(position, move, (4, 4, 4, 2)):
        step = step if sign > 0 else (size - step) % size
        moved.append(lax.rem(at + step, size) if step else at)
    return tuple(moved)


def block_terms(groups, extra_ref):
    square = (SPAN, SPAN)
    row, col = iota(square, 0), iota(square, 1)
    lower = row >= col
    lower_bf = jnp.where(lower, 1.0, 0.0).astype(BF16)
    items = []
    for group, (r_, k_, v_, p_, c_, base_, width) in enumerate(groups):
        for block in range(r_.shape[0] // SPAN):
            at = pl.ds(block * SPAN, SPAN)
            key = k_[at, :].astype(F32)
            unit = key * lax.rsqrt(head_sum(key * key, width) + KEY_EPSILON)
            removal = unit * jax.nn.sigmoid(c_[at, :].astype(F32))
            slow = jax.nn.sigmoid(p_[at, :].astype(F32))
            extra = extra_ref[pl.ds(block, 1), :]
            rate = 2.0 * base_[...]
            high, low = halves(slow)
            run_slow = nn(lower_bf, high) + nn(lower_bf, low)
            run_extra = jnp.sum(jnp.where(lower, extra, 0.0), axis=-1, keepdims=True)
            own_extra = jnp.sum(jnp.where(row == col, extra, 0.0), axis=-1, keepdims=True)
            running = run_extra - rate * run_slow
            own_log = own_extra - rate * slow
            centre = running[SPAN // 2 - 1 : SPAN // 2, :]
            ending = running[SPAN - 1 : SPAN, :]
            grown = running - centre
            write = removal * jnp.exp(-grown)
            items.append(
                dict(
                    group=group,
                    block=block,
                    width=width,
                    read=r_[at, :].astype(F32) * jnp.exp(grown),
                    query=unit * jnp.exp(grown - own_log),
                    write=write,
                    write_end=write * jnp.exp(ending - centre),
                    value=v_[at, :].astype(F32),
                    centre=jnp.exp(centre),
                    ending=jnp.exp(ending),
                )
            )
    return items


def spread(item, x):
    if len(item["parts"]) == 1:
        return x
    first = iota(x.shape, 1) % SPAN < HEAD_SIZE_FIRST
    return jnp.concatenate([jnp.where(first, x, 0.0), jnp.where(first, 0.0, x)], axis=0)


def joined(item, name):
    return jnp.concatenate([part[name] for part in item["parts"]], axis=1)


def block_steps(items):
    square = (SPAN, SPAN)
    row, col = iota(square, 0), iota(square, 1)
    strict = row > col
    lower = row >= col
    eye = jnp.where(row == col, 1.0, 0.0)
    solves = []
    for item in items:
        lane = col < item["width"]
        masks = [None] if item["width"] == SPAN else [lane, jnp.logical_not(lane)]
        item["parts"] = []
        for mask in masks:
            query = item["query"] if mask is None else jnp.where(mask, item["query"], 0.0)
            read = item["read"] if mask is None else jnp.where(mask, item["read"], 0.0)
            both = dot(nt, jnp.concatenate([query, read], axis=0), item["write"])
            part = dict(
                coupling=jnp.where(strict, both[:SPAN], 0.0),
                reading=jnp.where(lower, both[SPAN:], 0.0),
            )
            item["parts"].append(part)
            solves.append(part)
    size = 1
    while size < SPAN:
        near = ((row // (2 * size)) == (col // (2 * size))) & ((row // size) > (col // size))
        for part in solves:
            step = jnp.where(near, part["coupling"], 0.0)
            if size == 1:
                part["inverse"] = eye - step
            else:
                inverse = part["inverse"]
                part["inverse"] = inverse - dot(nn, dot(nn, inverse, step), inverse)
        size *= 2
    same_head = (row < HEAD_SIZE_FIRST) == (col < HEAD_SIZE_FIRST)
    for item in items:
        right = jnp.concatenate([item["value"], -item["query"]], axis=1)
        solved = dot(nn, joined(item, "inverse"), spread(item, right))
        item["solved"] = solved
        scaled = jnp.concatenate([solved[:, :SPAN], solved[:, SPAN:] * item["centre"]], axis=1)
        step = dot(nn, item["write_end"].T, scaled)
        diagonal = jnp.where(row == col, item["ending"], 0.0)
        step = step + jnp.concatenate([jnp.zeros(square, F32), diagonal], axis=1)
        if item["width"] < SPAN:
            step = jnp.where(jnp.concatenate([same_head, same_head], axis=1), step, 0.0)
        item["step"] = step


def block_chain(items):
    held = None
    for item in items:
        item["held"] = held
        step = item["step"]
        if held is None:
            held = step
        else:
            held = dot(nn, step[:, SPAN:], held)
            held = jnp.concatenate([held[:, :SPAN] + step[:, :SPAN], held[:, SPAN:]], axis=1)
    return held


def block_reads(items, read_ref, map_ref):
    for item in items:
        given = dot(nn, joined(item, "reading"), spread(item, item["solved"]))
        local_read = given[:, :SPAN]
        state_read = (item["read"] + given[:, SPAN:]) * item["centre"]
        at = pl.ds(item["block"] * SPAN, SPAN)
        if item["held"] is not None:
            out = dot(nn, state_read, item["held"])
            local_read = local_read + out[:, :SPAN]
            state_read = out[:, SPAN:]
        read_ref[item["group"], at, :] = local_read
        map_ref[item["group"], at, :] = state_read.astype(BF16)


def pack(ref, first, second):
    ref[0:64, :] = (first[:64, :] + first[64:, :]).astype(BF16)
    ref[64:192, :] = second.astype(BF16)


def unpack(packed):
    square = (LANES, 2 * LANES)
    same = (iota(square, 0) < 64) == (iota(square, 1) % LANES < 64)
    top = packed[0:64, :]
    first = jnp.where(same, jnp.concatenate([top, top], axis=0), jnp.zeros((), BF16))
    return first, packed[64:192, :]


def follow(step, held):
    high, low = halves(held)
    return nn(step[:, LANES:], high) + nn(step[:, LANES:], low)


def compose(step, held):
    moved = follow(step, held)
    return jnp.concatenate(
        [moved[:, :LANES] + step[:, :LANES].astype(F32), moved[:, LANES:]], axis=1
    )


def layer_kernel(
    r_a,
    k_a,
    v_a,
    p_a,
    c_a,
    base_a,
    gain_a,
    r_b,
    k_b,
    v_b,
    p_b,
    c_b,
    base_b,
    gain_b,
    extra,
    gain,
    index,
    weights,
    slot_of,
    residual,
    weight_a,
    weight_b,
    gate,
    up,
    down,
    shared_gate,
    shared_up,
    shared_down,
    out,
    residual_v,
    weight_v,
    gate_v,
    up_v,
    down_v,
    shared_gate_v,
    shared_up_v,
    shared_down_v,
    read_v,
    map_v,
    rows_v,
    columns_v,
    message,
    total,
    enter_v,
    own,
    pair_out,
    pair_in,
    ring_out,
    ring_in,
    base,
    sent,
    arrived,
    back,
    returned,
    chunk_v,
    hidden,
    match_high,
    match_low,
    load_sem,
    row_send,
    row_recv,
    col_send,
    col_recv,
    pair_send,
    pair_recv,
    ring_send,
    ring_recv,
    out_send,
    out_recv,
    back_send,
    back_recv,
):
    z, x, y, c = position = tuple(lax.axis_index(name) for name in ALL)
    devices = len(MOVES)
    barrier = pltpu.get_barrier_semaphore()
    for move in LINES:
        pl.semaphore_signal(
            barrier, inc=1, device_id=shift(position, move, 1), device_id_type=MESH
        )
    pairs = (
        (weight_a, weight_v.at[pl.ds(0, LANES)]),
        (weight_b, weight_v.at[pl.ds(LANES, LANES)]),
        (residual, residual_v),
        (shared_gate, shared_gate_v),
        (shared_up, shared_up_v),
        (shared_down, shared_down_v),
        (gate, gate_v),
        (up, up_v),
        (down, down_v),
    )
    loads = [pltpu.make_async_copy(a, b, load_sem.at[k]) for k, (a, b) in enumerate(pairs)]
    for load in loads:
        load.start()

    def remote(src, dst, send, recv, goal):
        return pltpu.make_async_remote_copy(
            src_ref=src,
            dst_ref=dst,
            send_sem=send,
            recv_sem=recv,
            device_id=goal,
            device_id_type=MESH,
        )

    items = block_terms(
        (
            (r_a, k_a, v_a, p_a, c_a, base_a, HEAD_SIZE_FIRST),
            (r_b, k_b, v_b, p_b, c_b, base_b, SPAN),
        ),
        extra,
    )
    block_steps(items)
    chains = [[item for item in items if item["group"] == group] for group in range(2)]
    pack(message, *[block_chain(chain) for chain in chains])
    pl.semaphore_wait(barrier, len(LINES))

    def row_copy(d):
        goal = (z, lax.rem(x + d, 4), y, c)
        return remote(message, rows_v.at[d], row_send.at[d], row_recv.at[d], goal)

    def col_copy(d):
        goal = (lax.rem(z + d, 4), x, y, c)
        return remote(total, columns_v.at[d], col_send.at[d], col_recv.at[d], goal)

    for d in (2, 1, 3):
        row_copy(d).start()
    rows_v[0] = message[...]
    for chain in chains:
        block_reads(chain, read_v, map_v)

    square = (LANES, 2 * LANES)
    unit_step = jnp.where(iota(square, 0) + LANES == iota(square, 1), 1.0, 0.0)
    inside = [unit_step, unit_step]
    running = [unit_step, unit_step]
    for d in range(1, 4):
        row_copy(d).wait()
    for k in range(4):
        pair = unpack(rows_v[lax.rem(x - k + 4, 4)])
        inside = [jnp.where(x == k, now, old) for now, old in zip(running, inside)]
        if k == 0:
            running = [p.astype(F32) for p in pair]
        else:
            running = [compose(p, r) for p, r in zip(pair, running)]
    pack(total, *running)
    for d in (2, 1, 3):

        @pl.when(z + d < 4)
        def _():
            col_copy(d).start()

    enter_v[...] = jnp.zeros_like(enter_v)
    for k in range(3):

        @pl.when(k < z)
        def _():
            d = z - k
            remote(
                total, columns_v.at[d], col_send.at[d], col_recv.at[d], (k, x, y, c)
            ).wait_recv()
            for group, step in enumerate(unpack(columns_v[d])):
                enter_v[group] = follow(step, enter_v[group]) + step[:, :LANES].astype(F32)

    entering = []
    for group, step in enumerate(inside):
        enter = dot3(nn, step[:, LANES:], enter_v[group]) + step[:, :LANES]
        entering.append(halves(enter))

    rows, width = out.shape
    half = width // 2
    partner = (z, x, y, 1 - c)
    right, left = (z, x, lax.rem(y + 1, 4), c), (z, x, lax.rem(y + 3, 4), c)

    def pair_copy(d):
        return remote(pair_out.at[d], pair_in.at[d], pair_send.at[d], pair_recv.at[d], partner)

    def ring_copy(k):
        return remote(
            ring_out.at[k],
            ring_in.at[k],
            ring_send.at[k],
            ring_recv.at[k],
            right if k % 2 == 0 else left,
        )

    square = (LANES, LANES)
    row, col = iota(square, 0), iota(square, 1)
    for load in loads[:2]:
        load.wait()
    for d in (2, 1, 3, 0):
        start = lax.rem(y + d, 4) * (2 * rows)
        theirs = pl.ds(pl.multiple_of(start + (1 - c) * rows, rows), rows)
        mine = pl.ds(pl.multiple_of(start + c * rows, rows), rows)
        mixed = []
        for group, (head_gain, size) in enumerate(((gain_a, HEAD_SIZE_FIRST), (gain_b, SPAN))):
            mean = jnp.where((row // size) == (col // size), 1.0 / size, 0.0).astype(BF16)
            high, low = entering[group]
            maps = jnp.concatenate([map_v[group, theirs, :], map_v[group, mine, :]], axis=0)
            reads = jnp.concatenate([read_v[group, theirs, :], read_v[group, mine, :]], axis=0)
            readout = reads + nn(maps, high) + nn(maps, low)
            high, low = halves(readout)
            centred = readout - (nn(high, mean) + nn(low, mean))
            high, low = halves(centred * centred)
            variance = nn(high, mean) + nn(low, mean)
            mixed.append((centred * lax.rsqrt(variance + HEAD_EPSILON) * head_gain[...]).astype(BF16))
        both = jnp.concatenate(mixed, axis=1)
        for at in range(0, width, 512):
            product = nn(both, weight_v[:, at : at + 512])
            pair_out[d, :, at : at + 512] = product[:rows].astype(BF16)
            own[d, :, at : at + 512] = product[rows:]
        pair_copy(d).start()

    pair_copy(2).wait()
    for k in range(2):
        at = slice(k * half, (k + 1) * half)
        ring_out[k] = (own[2, :, at] + pair_in[2, :, at].astype(F32)).astype(BF16)
    for k in range(2):
        ring_copy(k).start()
    for k, d, at, keep in (
        (2, 1, slice(half, width), slice(0, half)),
        (3, 3, slice(0, half), slice(half, width)),
    ):
        pair_copy(d).wait()
        ring_out[k] = (own[d, :, at] + pair_in[d, :, at].astype(F32)).astype(BF16)
        ring_copy(k).start()
        own[d, :, keep] += pair_in[d, :, keep].astype(F32)
    pair_copy(0).wait()
    loads[2].wait()
    base[...] = residual_v[...].astype(F32) + (own[0] + pair_in[0].astype(F32))
    for k, d, keep in ((4, 1, slice(0, half)), (5, 3, slice(half, width))):
        ring_copy(k - 4).wait()
        ring_out[k] = (own[d, :, keep] + ring_in[k - 4].astype(F32)).astype(BF16)
        ring_copy(k).start()
    for k, at in (
        (2, slice(half, width)),
        (3, slice(0, half)),
        (4, slice(0, half)),
        (5, slice(half, width)),
    ):
        ring_copy(k).wait()
        base[:, at] += ring_in[k].astype(F32)

    def unit(k):
        return pl.ds(k * UNIT, UNIT)

    def out_copy(k):
        return remote(
            sent.at[unit(k)],
            arrived.at[unit(k)],
            out_send.at[k],
            out_recv.at[k],
            shift(position, MOVES[k], 1),
        )

    def back_copy(k):
        return remote(
            back.at[unit(k)],
            returned.at[unit(k)],
            back_send.at[k],
            back_recv.at[k],
            shift(position, MOVES[k], -1),
        )

    wide = base[...].astype(BF16).astype(F32)
    mean = jnp.mean(wide * wide, axis=-1, keepdims=True)
    normed = (wide * lax.rsqrt(mean + NORM_EPSILON) * gain[...]).astype(BF16)
    base[...] = wide
    part = width // PARTS
    stacked = jnp.concatenate([normed[:, q * part : (q + 1) * part] for q in range(PARTS)], axis=0)

    ids = index[...]
    relative = (
        ((((ids >> 5) - z) & 3) << 5)
        + ((((ids >> 3) - x) & 3) << 3)
        + ((((ids >> 1) - y) & 3) << 1)
        + ((ids - c) & 1)
    )
    experts = iota((LANES, rows), 0)
    chosen = jnp.zeros((LANES, rows), F32)
    scale = jnp.zeros((LANES, rows), F32)
    for k in range(ids.shape[0]):
        here = relative[k : k + 1, :] == experts
        chosen += jnp.where(here, 1.0, 0.0)
        scale += jnp.where(here, weights[k : k + 1, :], 0.0)
    chosen = nn(chosen.T.astype(BF16), slot_of[...])
    high, low = [nn(term, slot_of[...]).astype(BF16) for term in halves(scale.T)]
    earlier = jnp.where(iota((rows, rows), 0) > iota((rows, rows), 1), 1.0, 0.0).astype(BF16)
    rank = nn(earlier, chosen.astype(BF16))
    code = jnp.concatenate([(chosen * (rank + 1.0)).astype(BF16)] * PARTS, axis=0)
    high, low = [jnp.concatenate([term] * PARTS, axis=0) for term in (high, low)]

    groups = sent.shape[0] // GROUP
    per = GROUP // UNIT
    shape = (GROUP, PARTS * rows)
    place = iota(shape, 0) % UNIT
    fits = (place // SLOTS) == (iota(shape, 1) // rows)
    wanted = (place % SLOTS + 1).astype(F32)

    def select(k):
        found = (iota((GROUP, LANES), 0) + GROUP * k) // UNIT == iota((GROUP, LANES), 1)
        return jnp.where(found, 1.0, 0.0).astype(BF16)

    span = groups // CHUNKS

    def chunk_slots(k):
        return range(per * span * k, min(per * span * (k + 1), devices - 1))

    def launch(k):
        for slot in range(per * k, min(per * (k + 1), devices - 1)):
            out_copy(slot).start()

    for k in range(groups):
        found = nt(select(k), code)
        taken = jnp.where(fits & (found == wanted), 1.0, 0.0).astype(BF16)
        sent[GROUP * k : GROUP * (k + 1), :] = nn(taken, stacked).astype(BF16)
        if 0 < k <= WINDOW * span:
            launch(k - 1)
    if WINDOW * span >= groups:
        launch(groups - 1)
    arrived[unit(devices - 1), :] = sent[unit(devices - 1), :]

    for load in loads[3:5]:
        load.wait()
    gate_val = nn(normed, shared_gate_v[...])
    up_val = nn(normed, shared_up_v[...])
    shared = (gate_val * jax.nn.sigmoid(gate_val) * up_val).astype(BF16)
    loads[5].wait()
    for at in range(0, width, 512):
        base[:, at : at + 512] += nn(shared, shared_down_v[:, at : at + 512])

    shape = (PARTS * rows, GROUP)
    place = iota(shape, 1) % UNIT
    fits = (place // SLOTS) == (iota(shape, 0) // rows)
    wanted = (place % SLOTS + 1).astype(F32)
    for k in range(groups):
        chosen_here = select(k)
        match = fits & (nt(code, chosen_here) == wanted)
        match_high[k] = jnp.where(match, nt(high, chosen_here), 0.0).astype(BF16)
        match_low[k] = jnp.where(match, nt(low, chosen_here), 0.0).astype(BF16)

    a, b = iota((GROUP, GROUP), 0), iota((GROUP, GROUP), 1)
    here = (b % UNIT // SLOTS) * 64 + (b // UNIT) * SLOTS + b % SLOTS
    order = jnp.where(a == here, 1.0, 0.0).astype(BF16)
    there = (a % UNIT // SLOTS) * 64 + (a // UNIT) * SLOTS + a % SLOTS
    order_back = jnp.where(b == there, 1.0, 0.0).astype(BF16)
    for load in loads[6:]:
        load.wait()

    for chunk in range(CHUNKS):
        for slot in chunk_slots(chunk):
            out_copy(slot).wait_recv()
        for g in range(span):
            k = chunk * span + g
            sorted_ = nn(order, arrived[GROUP * k : GROUP * (k + 1), :]).astype(BF16)
            for q in range(PARTS):
                chunk_v[64 * g : 64 * (g + 1), q * part : (q + 1) * part] = sorted_[
                    64 * q : 64 * (q + 1)
                ]
        for at in range(0, hidden.shape[1], 256):
            gate_val = nn(chunk_v[...], gate_v[:, at : at + 256])
            up_val = nn(chunk_v[...], up_v[:, at : at + 256])
            hidden[:, at : at + 256] = (gate_val * jax.nn.sigmoid(gate_val) * up_val).astype(BF16)
        for at in range(0, width, 512):
            chunk_v[:, at : at + 512] = nn(hidden[...], down_v[:, at : at + 512]).astype(BF16)
        for g in range(span):
            k = chunk * span + g
            gathered = jnp.concatenate(
                [chunk_v[64 * g : 64 * (g + 1), q * part : (q + 1) * part] for q in range(PARTS)],
                axis=0,
            )
            back[GROUP * k : GROUP * (k + 1), :] = nn(order_back, gathered).astype(BF16)
        for slot in chunk_slots(chunk):
            back_copy(slot).start()
        if chunk + WINDOW < CHUNKS:
            for slot in chunk_slots(chunk):
                out_copy(slot).wait_send()
            for slot in chunk_slots(chunk + WINDOW):
                out_copy(slot).start()
    returned[unit(devices - 1), :] = back[unit(devices - 1), :]

    routed = jnp.zeros((PARTS * rows, part), F32)
    for k in range(groups):
        for slot in range(per * k, min(per * (k + 1), devices - 1)):
            back_copy(slot).wait_recv()
        block = returned[GROUP * k : GROUP * (k + 1), :]
        routed += nn(match_high[k], block) + nn(match_low[k], block)
    for q in range(PARTS):
        at = slice(q * part, (q + 1) * part)
        out[:, at] = (base[:, at] + routed[q * rows : (q + 1) * rows, :]).astype(BF16)
    for d in (2, 1, 3):

        @pl.when(z + d < 4)
        def _():
            col_copy(d).wait_send()

    for chunk in range(CHUNKS):
        for slot in chunk_slots(chunk):
            if chunk + WINDOW >= CHUNKS:
                out_copy(slot).wait_send()
            back_copy(slot).wait_send()


def slot_table():
    devices = len(MOVES)
    table = np.zeros((devices, devices), np.float32)
    for slot, (dz, dx, dy, dc) in enumerate(MOVES):
        table[((dz * 4 + dx) * 4 + dy) * 2 + dc, slot] = 1.0
    return jnp.asarray(table, BF16)


def layer_call(small, large):
    rows, width = large[0].shape
    long = small[0].shape[0]
    gate = large[3]
    devices = len(MOVES)
    part = width // PARTS
    slots = pltpu.VMEM((devices * UNIT, part), BF16)
    match = pltpu.VMEM((devices * UNIT // GROUP, PARTS * rows, GROUP), BF16)
    chunk_rows = devices * SLOTS // CHUNKS
    packed = (192, 2 * LANES)
    scratch = (
        [pltpu.VMEM((rows, width), BF16), pltpu.VMEM((2 * LANES, width), BF16)]
        + [pltpu.VMEM(a.shape, BF16) for a in large[3:]]
        + [
            pltpu.VMEM((2, long, LANES), F32),
            pltpu.VMEM((2, long, LANES), BF16),
            pltpu.VMEM((4, *packed), BF16),
            pltpu.VMEM((4, *packed), BF16),
            pltpu.VMEM(packed, BF16),
            pltpu.VMEM(packed, BF16),
            pltpu.VMEM((2, LANES, LANES), F32),
            pltpu.VMEM((4, rows, width), F32),
            pltpu.VMEM((4, rows, width), BF16),
            pltpu.VMEM((4, rows, width), BF16),
            pltpu.VMEM((6, rows, width // 2), BF16),
            pltpu.VMEM((6, rows, width // 2), BF16),
            pltpu.VMEM((rows, width), F32),
        ]
        + [slots] * 4
        + [
            pltpu.VMEM((chunk_rows, width), BF16),
            pltpu.VMEM((chunk_rows, gate.shape[1]), BF16),
            match,
            match,
            pltpu.SemaphoreType.DMA((9,)),
        ]
        + [pltpu.SemaphoreType.DMA((4,))] * 6
        + [pltpu.SemaphoreType.DMA((6,))] * 2
        + [pltpu.SemaphoreType.DMA((devices,))] * 4
    )
    return pl.pallas_call(
        layer_kernel,
        out_shape=jax.ShapeDtypeStruct((rows, width), BF16),
        in_specs=[pl.BlockSpec(memory_space=pltpu.VMEM)] * len(small)
        + [pl.BlockSpec(memory_space=pl.ANY)] * len(large),
        out_specs=pl.BlockSpec(memory_space=pltpu.VMEM),
        scratch_shapes=scratch,
        compiler_params=pltpu.CompilerParams(
            collective_id=0, has_side_effects=True, vmem_limit_bytes=60 * 1024 * 1024
        ),
        name="layer",
    )(*small, *large)


def local(
    residual,
    receptance_first,
    key_first_group,
    value_first_group,
    decay_preact_first,
    context_rate_first,
    decay_base_first,
    head_scale_first,
    receptance_second,
    key_second_group,
    value_second_group,
    decay_preact_second,
    context_rate_second,
    decay_base_second,
    head_scale_second,
    decay_extra_log,
    output_weight_first,
    output_weight_second,
    feedforward_gain,
    routed_expert_index,
    routed_expert_weight,
    expert_gate_weight,
    expert_up_weight,
    expert_down_weight,
    shared_gate_weight,
    shared_up_weight,
    shared_down_weight,
):
    small = (
        receptance_first,
        key_first_group,
        value_first_group,
        decay_preact_first,
        context_rate_first,
        decay_base_first[None, :],
        head_scale_first[None, :],
        receptance_second,
        key_second_group,
        value_second_group,
        decay_preact_second,
        context_rate_second,
        decay_base_second[None, :],
        head_scale_second[None, :],
        decay_extra_log.reshape(-1, SPAN),
        feedforward_gain[None, :],
        routed_expert_index.T,
        routed_expert_weight.T,
        slot_table(),
    )
    large = (
        residual,
        output_weight_first,
        output_weight_second,
        expert_gate_weight[0],
        expert_up_weight[0],
        expert_down_weight[0],
        shared_gate_weight,
        shared_up_weight,
        shared_down_weight,
    )
    return layer_call(small, large)


def solution(mesh):
    finer = Mesh(mesh.devices.reshape(4, 4, 4, 2), ALL)
    sp, tp = (Z, X), (Y, C)
    heads = (P(sp, tp),) * 5 + (P(tp),) * 2
    placed = (
        (P(ALL, None),)
        + heads
        + heads
        + (P(sp), P(tp, None), P(tp, None), P(), P(ALL, None), P(ALL, None))
        + (P(ALL, None, None),) * 3
        + (P(),) * 3
    )
    return jax.shard_map(
        local, mesh=finer, in_specs=placed, out_specs=P(ALL, None), check_vma=False
    )
```

```python
import functools
import itertools

import jax
import jax.numpy as jnp
import numpy as np
from jax import lax
from jax.experimental import pallas as pl
from jax.experimental.pallas import tpu as pltpu
from jax.sharding import Mesh
from jax.sharding import PartitionSpec as P

F32, BF16 = jnp.float32, jnp.bfloat16
SPAN = 128
LANES = 128
HEAD_SIZE_FIRST = 64
KEY_EPSILON = 1e-06
HEAD_EPSILON = 0.00064
NORM_EPSILON = 1e-06
Z, X, Y, C = "z", "x", "y", "core"
ALL = (Z, X, Y, C)
MESH = pl.DeviceIdType.MESH
SLOTS = 4
PARTS = 4
UNIT = SLOTS * PARTS
GROUP = 256
CHUNKS = 8
WINDOW = 8


def distance(move):
    return sum(min(step, 4 - step) for step in move[:3])


MOVES = [[3, 3, 3, 1], [1, 0, 3, 1], [2, 2, 3, 0], [1, 1, 1, 0], [1, 2, 1, 1], [0, 0, 2, 1], [1, 1, 3, 0], [3, 3, 2, 0], [1, 1, 2, 0], [1, 0, 2, 1], [2, 3, 3, 1], [0, 1, 3, 1], [3, 3, 1, 0], [3, 2, 0, 1], [0, 2, 3, 0], [3, 0, 0, 0], [0, 1, 0, 0], [0, 2, 0, 1], [0, 3, 0, 1], [1, 1, 0, 0], [0, 2, 2, 1], [3, 2, 2, 0], [3, 1, 2, 0], [2, 2, 0, 1], [3, 0, 2, 0], [0, 2, 3, 1], [0, 1, 1, 0], [2, 3, 0, 0], [2, 2, 3, 1], [3, 0, 3, 0], [1, 2, 2, 0], [2, 2, 0, 0], [2, 3, 3, 0], [1, 1, 3, 1], [1, 0, 1, 0], [0, 1, 1, 1], [0, 0, 3, 1], [1, 3, 3, 0], [2, 1, 1, 1], [0, 0, 3, 0], [2, 1, 2, 1], [1, 0, 2, 0], [2, 0, 2, 1], [0, 1, 2, 0], [1, 3, 2, 0], [3, 2, 0, 0], [1, 2, 2, 1], [1, 2, 0, 0], [2, 0, 1, 1], [0, 3, 3, 1], [2, 1, 0, 0], [3, 1, 1, 0], [0, 3, 1, 0], [3, 1, 3, 0], [1, 0, 0, 0], [2, 2, 1, 1], [0, 2, 1, 1], [0, 2, 2, 0], [2, 3, 0, 1], [2, 0, 1, 0], [2, 1, 1, 0], [2, 1, 3, 1], [3, 3, 0, 1], [2, 2, 2, 1], [2, 0, 0, 1], [1, 1, 1, 1], [3, 3, 0, 0], [3, 3, 3, 0], [0, 3, 0, 0], [3, 1, 3, 1], [1, 2, 3, 0], [2, 3, 2, 0], [1, 0, 3, 0], [1, 3, 1, 1], [2, 2, 1, 0], [3, 1, 0, 1], [1, 1, 2, 1], [3, 0, 0, 1], [2, 0, 3, 1], [3, 2, 3, 1], [1, 3, 0, 1], [0, 3, 2, 1], [2, 0, 2, 0], [2, 3, 1, 1], [1, 2, 3, 1], [0, 3, 2, 0], [3, 2, 1, 0], [0, 0, 1, 0], [2, 0, 3, 0], [3, 2, 1, 1], [3, 1, 0, 0], [0, 0, 1, 1], [3, 3, 2, 1], [1, 1, 0, 1], [0, 1, 3, 0], [2, 1, 2, 0], [0, 3, 3, 0], [2, 3, 2, 1], [1, 0, 1, 1], [3, 2, 2, 1], [2, 3, 1, 0], [0, 0, 0, 1], [3, 0, 1, 1], [3, 2, 3, 0], [2, 1, 3, 0], [1, 3, 0, 0], [1, 2, 1, 0], [3, 1, 1, 1], [0, 0, 2, 0], [1, 3, 3, 1], [0, 1, 2, 1], [0, 3, 1, 1], [3, 0, 2, 1], [1, 2, 0, 1], [2, 2, 2, 0], [1, 3, 2, 1], [1, 3, 1, 0], [3, 3, 1, 1], [2, 0, 0, 0], [0, 2, 0, 0], [1, 0, 0, 1], [0, 1, 0, 1], [3, 0, 1, 0], [3, 0, 3, 1], [3, 1, 2, 1], [2, 1, 0, 1], [0, 2, 1, 0], [0, 0, 0, 0]]
MOVES = [tuple(move) for move in MOVES]


LINES = [move for move in MOVES if sum(step > 0 for step in move) == 1]


def nn(a, b):
    return lax.dot_general(a, b, (((1,), (0,)), ((), ())), preferred_element_type=F32)


def nt(a, b):
    return lax.dot_general(a, b, (((1,), (1,)), ((), ())), preferred_element_type=F32)


def halves(x):
    high = x.astype(BF16)
    return high, (x - high.astype(F32)).astype(BF16)


def dot(f, a, b):
    return f(a.astype(BF16), b.astype(BF16))


def dot3(f, a, b):
    ah, al = halves(a)
    bh, bl = halves(b)
    return f(ah, bh) + (f(ah, bl) + f(al, bh))


def iota(shape, dim):
    return lax.broadcasted_iota(jnp.int32, shape, dim)


def head_sum(x, width):
    if width == LANES:
        return jnp.sum(x, axis=-1, keepdims=True)
    lane = iota(x.shape, 1)
    left = jnp.sum(jnp.where(lane < width, x, 0.0), axis=-1, keepdims=True)
    right = jnp.sum(jnp.where(lane < width, 0.0, x), axis=-1, keepdims=True)
    return jnp.where(lane < width, left, right)


def shift(position, move, sign):
    moved = []
    for at, step, size in zip(position, move, (4, 4, 4, 2)):
        step = step if sign > 0 else (size - step) % size
        moved.append(lax.rem(at + step, size) if step else at)
    return tuple(moved)


def block_terms(groups, extra_ref):
    square = (SPAN, SPAN)
    row, col = iota(square, 0), iota(square, 1)
    lower = row >= col
    lower_bf = jnp.where(lower, 1.0, 0.0).astype(BF16)
    items = []
    for group, (r_, k_, v_, p_, c_, base_, width) in enumerate(groups):
        for block in range(r_.shape[0] // SPAN):
            at = pl.ds(block * SPAN, SPAN)
            key = k_[at, :].astype(F32)
            unit = key * lax.rsqrt(head_sum(key * key, width) + KEY_EPSILON)
            removal = unit * jax.nn.sigmoid(c_[at, :].astype(F32))
            slow = jax.nn.sigmoid(p_[at, :].astype(F32))
            extra = extra_ref[pl.ds(block, 1), :]
            rate = 2.0 * base_[...]
            high, low = halves(slow)
            run_slow = nn(lower_bf, high) + nn(lower_bf, low)
            run_extra = jnp.sum(jnp.where(lower, extra, 0.0), axis=-1, keepdims=True)
            own_extra = jnp.sum(jnp.where(row == col, extra, 0.0), axis=-1, keepdims=True)
            running = run_extra - rate * run_slow
            own_log = own_extra - rate * slow
            centre = running[SPAN // 2 - 1 : SPAN // 2, :]
            ending = running[SPAN - 1 : SPAN, :]
            grown = running - centre
            write = removal * jnp.exp(-grown)
            items.append(
                dict(
                    group=group,
                    block=block,
                    width=width,
                    read=r_[at, :].astype(F32) * jnp.exp(grown),
                    query=unit * jnp.exp(grown - own_log),
                    write=write,
                    write_end=write * jnp.exp(ending - centre),
                    value=v_[at, :].astype(F32),
                    centre=jnp.exp(centre),
                    ending=jnp.exp(ending),
                )
            )
    return items


def spread(item, x):
    if len(item["parts"]) == 1:
        return x
    first = iota(x.shape, 1) % SPAN < HEAD_SIZE_FIRST
    return jnp.concatenate([jnp.where(first, x, 0.0), jnp.where(first, 0.0, x)], axis=0)


def joined(item, name):
    return jnp.concatenate([part[name] for part in item["parts"]], axis=1)


def block_steps(items):
    square = (SPAN, SPAN)
    row, col = iota(square, 0), iota(square, 1)
    strict = row > col
    lower = row >= col
    eye = jnp.where(row == col, 1.0, 0.0)
    solves = []
    for item in items:
        lane = col < item["width"]
        masks = [None] if item["width"] == SPAN else [lane, jnp.logical_not(lane)]
        item["parts"] = []
        for mask in masks:
            query = item["query"] if mask is None else jnp.where(mask, item["query"], 0.0)
            read = item["read"] if mask is None else jnp.where(mask, item["read"], 0.0)
            both = dot(nt, jnp.concatenate([query, read], axis=0), item["write"])
            part = dict(
                coupling=jnp.where(strict, both[:SPAN], 0.0),
                reading=jnp.where(lower, both[SPAN:], 0.0),
            )
            item["parts"].append(part)
            solves.append(part)
    size = 1
    while size < SPAN:
        near = ((row // (2 * size)) == (col // (2 * size))) & ((row // size) > (col // size))
        for part in solves:
            step = jnp.where(near, part["coupling"], 0.0)
            if size == 1:
                part["inverse"] = eye - step
            else:
                inverse = part["inverse"]
                part["inverse"] = inverse - dot(nn, dot(nn, inverse, step), inverse)
        size *= 2
    same_head = (row < HEAD_SIZE_FIRST) == (col < HEAD_SIZE_FIRST)
    for item in items:
        right = jnp.concatenate([item["value"], -item["query"]], axis=1)
        solved = dot(nn, joined(item, "inverse"), spread(item, right))
        item["solved"] = solved
        scaled = jnp.concatenate([solved[:, :SPAN], solved[:, SPAN:] * item["centre"]], axis=1)
        step = dot(nn, item["write_end"].T, scaled)
        diagonal = jnp.where(row == col, item["ending"], 0.0)
        step = step + jnp.concatenate([jnp.zeros(square, F32), diagonal], axis=1)
        if item["width"] < SPAN:
            step = jnp.where(jnp.concatenate([same_head, same_head], axis=1), step, 0.0)
        item["step"] = step


def block_chain(items):
    held = None
    for item in items:
        item["held"] = held
        step = item["step"]
        if held is None:
            held = step
        else:
            held = dot(nn, step[:, SPAN:], held)
            held = jnp.concatenate([held[:, :SPAN] + step[:, :SPAN], held[:, SPAN:]], axis=1)
    return held


def block_reads(items, read_ref, map_ref):
    for item in items:
        given = dot(nn, joined(item, "reading"), spread(item, item["solved"]))
        local_read = given[:, :SPAN]
        state_read = (item["read"] + given[:, SPAN:]) * item["centre"]
        at = pl.ds(item["block"] * SPAN, SPAN)
        if item["held"] is not None:
            out = dot(nn, state_read, item["held"])
            local_read = local_read + out[:, :SPAN]
            state_read = out[:, SPAN:]
        read_ref[item["group"], at, :] = local_read
        map_ref[item["group"], at, :] = state_read.astype(BF16)


def pack(ref, first, second):
    ref[0:64, :] = (first[:64, :] + first[64:, :]).astype(BF16)
    ref[64:192, :] = second.astype(BF16)


def unpack(packed):
    square = (LANES, 2 * LANES)
    same = (iota(square, 0) < 64) == (iota(square, 1) % LANES < 64)
    top = packed[0:64, :]
    first = jnp.where(same, jnp.concatenate([top, top], axis=0), jnp.zeros((), BF16))
    return first, packed[64:192, :]


def follow(step, held):
    high, low = halves(held)
    return nn(step[:, LANES:], high) + nn(step[:, LANES:], low)


def compose(step, held):
    moved = follow(step, held)
    return jnp.concatenate(
        [moved[:, :LANES] + step[:, :LANES].astype(F32), moved[:, LANES:]], axis=1
    )


def layer_kernel(
    r_a,
    k_a,
    v_a,
    p_a,
    c_a,
    base_a,
    gain_a,
    r_b,
    k_b,
    v_b,
    p_b,
    c_b,
    base_b,
    gain_b,
    extra,
    gain,
    index,
    weights,
    slot_of,
    residual,
    weight_a,
    weight_b,
    gate,
    up,
    down,
    shared_gate,
    shared_up,
    shared_down,
    out,
    residual_v,
    weight_v,
    gate_v,
    up_v,
    down_v,
    shared_gate_v,
    shared_up_v,
    shared_down_v,
    read_v,
    map_v,
    rows_v,
    columns_v,
    message,
    total,
    enter_v,
    own,
    pair_out,
    pair_in,
    ring_out,
    ring_in,
    base,
    sent,
    arrived,
    back,
    returned,
    chunk_v,
    hidden,
    match_high,
    match_low,
    load_sem,
    row_send,
    row_recv,
    col_send,
    col_recv,
    pair_send,
    pair_recv,
    ring_send,
    ring_recv,
    out_send,
    out_recv,
    back_send,
    back_recv,
):
    z, x, y, c = position = tuple(lax.axis_index(name) for name in ALL)
    devices = len(MOVES)
    barrier = pltpu.get_barrier_semaphore()
    for move in LINES:
        pl.semaphore_signal(
            barrier, inc=1, device_id=shift(position, move, 1), device_id_type=MESH
        )
    pairs = (
        (weight_a, weight_v.at[pl.ds(0, LANES)]),
        (weight_b, weight_v.at[pl.ds(LANES, LANES)]),
        (residual, residual_v),
        (shared_gate, shared_gate_v),
        (shared_up, shared_up_v),
        (shared_down, shared_down_v),
        (gate, gate_v),
        (up, up_v),
        (down, down_v),
    )
    loads = [pltpu.make_async_copy(a, b, load_sem.at[k]) for k, (a, b) in enumerate(pairs)]
    for load in loads:
        load.start()

    def remote(src, dst, send, recv, goal):
        return pltpu.make_async_remote_copy(
            src_ref=src,
            dst_ref=dst,
            send_sem=send,
            recv_sem=recv,
            device_id=goal,
            device_id_type=MESH,
        )

    items = block_terms(
        (
            (r_a, k_a, v_a, p_a, c_a, base_a, HEAD_SIZE_FIRST),
            (r_b, k_b, v_b, p_b, c_b, base_b, SPAN),
        ),
        extra,
    )
    block_steps(items)
    chains = [[item for item in items if item["group"] == group] for group in range(2)]
    pack(message, *[block_chain(chain) for chain in chains])
    pl.semaphore_wait(barrier, len(LINES))

    def row_copy(d):
        goal = (z, lax.rem(x + d, 4), y, c)
        return remote(message, rows_v.at[d], row_send.at[d], row_recv.at[d], goal)

    def col_copy(d):
        goal = (lax.rem(z + d, 4), x, y, c)
        return remote(total, columns_v.at[d], col_send.at[d], col_recv.at[d], goal)

    for d in (2, 1, 3):
        row_copy(d).start()
    rows_v[0] = message[...]
    for chain in chains:
        block_reads(chain, read_v, map_v)

    square = (LANES, 2 * LANES)
    unit_step = jnp.where(iota(square, 0) + LANES == iota(square, 1), 1.0, 0.0)
    inside = [unit_step, unit_step]
    running = [unit_step, unit_step]
    for d in range(1, 4):
        row_copy(d).wait()
    for k in range(4):
        pair = unpack(rows_v[lax.rem(x - k + 4, 4)])
        inside = [jnp.where(x == k, now, old) for now, old in zip(running, inside)]
        if k == 0:
            running = [p.astype(F32) for p in pair]
        else:
            running = [compose(p, r) for p, r in zip(pair, running)]
    pack(total, *running)
    for d in (2, 1, 3):

        @pl.when(z + d < 4)
        def _():
            col_copy(d).start()

    enter_v[...] = jnp.zeros_like(enter_v)
    for k in range(3):

        @pl.when(k < z)
        def _():
            d = z - k
            remote(
                total, columns_v.at[d], col_send.at[d], col_recv.at[d], (k, x, y, c)
            ).wait_recv()
            for group, step in enumerate(unpack(columns_v[d])):
                enter_v[group] = follow(step, enter_v[group]) + step[:, :LANES].astype(F32)

    entering = []
    for group, step in enumerate(inside):
        enter = dot3(nn, step[:, LANES:], enter_v[group]) + step[:, :LANES]
        entering.append(halves(enter))

    rows, width = out.shape
    half = width // 2
    partner = (z, x, y, 1 - c)
    right, left = (z, x, lax.rem(y + 1, 4), c), (z, x, lax.rem(y + 3, 4), c)

    def pair_copy(d):
        return remote(pair_out.at[d], pair_in.at[d], pair_send.at[d], pair_recv.at[d], partner)

    def ring_copy(k):
        return remote(
            ring_out.at[k],
            ring_in.at[k],
            ring_send.at[k],
            ring_recv.at[k],
            right if k % 2 == 0 else left,
        )

    square = (LANES, LANES)
    row, col = iota(square, 0), iota(square, 1)
    for load in loads[:2]:
        load.wait()
    for d in (2, 1, 3, 0):
        start = lax.rem(y + d, 4) * (2 * rows)
        theirs = pl.ds(pl.multiple_of(start + (1 - c) * rows, rows), rows)
        mine = pl.ds(pl.multiple_of(start + c * rows, rows), rows)
        mixed = []
        for group, (head_gain, size) in enumerate(((gain_a, HEAD_SIZE_FIRST), (gain_b, SPAN))):
            mean = jnp.where((row // size) == (col // size), 1.0 / size, 0.0).astype(BF16)
            high, low = entering[group]
            maps = jnp.concatenate([map_v[group, theirs, :], map_v[group, mine, :]], axis=0)
            reads = jnp.concatenate([read_v[group, theirs, :], read_v[group, mine, :]], axis=0)
            readout = reads + nn(maps, high) + nn(maps, low)
            high, low = halves(readout)
            centred = readout - (nn(high, mean) + nn(low, mean))
            high, low = halves(centred * centred)
            variance = nn(high, mean) + nn(low, mean)
            mixed.append((centred * lax.rsqrt(variance + HEAD_EPSILON) * head_gain[...]).astype(BF16))
        both = jnp.concatenate(mixed, axis=1)
        for at in range(0, width, 512):
            product = nn(both, weight_v[:, at : at + 512])
            pair_out[d, :, at : at + 512] = product[:rows].astype(BF16)
            own[d, :, at : at + 512] = product[rows:]
        pair_copy(d).start()

    pair_copy(2).wait()
    for k in range(2):
        at = slice(k * half, (k + 1) * half)
        ring_out[k] = (own[2, :, at] + pair_in[2, :, at].astype(F32)).astype(BF16)
    for k in range(2):
        ring_copy(k).start()
    for k, d, at, keep in (
        (2, 1, slice(half, width), slice(0, half)),
        (3, 3, slice(0, half), slice(half, width)),
    ):
        pair_copy(d).wait()
        ring_out[k] = (own[d, :, at] + pair_in[d, :, at].astype(F32)).astype(BF16)
        ring_copy(k).start()
        own[d, :, keep] += pair_in[d, :, keep].astype(F32)
    pair_copy(0).wait()
    loads[2].wait()
    base[...] = residual_v[...].astype(F32) + (own[0] + pair_in[0].astype(F32))
    for k, d, keep in ((4, 1, slice(0, half)), (5, 3, slice(half, width))):
        ring_copy(k - 4).wait()
        ring_out[k] = (own[d, :, keep] + ring_in[k - 4].astype(F32)).astype(BF16)
        ring_copy(k).start()
    for k, at in (
        (2, slice(half, width)),
        (3, slice(0, half)),
        (4, slice(0, half)),
        (5, slice(half, width)),
    ):
        ring_copy(k).wait()
        base[:, at] += ring_in[k].astype(F32)

    def unit(k):
        return pl.ds(k * UNIT, UNIT)

    def out_copy(k):
        return remote(
            sent.at[unit(k)],
            arrived.at[unit(k)],
            out_send.at[k],
            out_recv.at[k],
            shift(position, MOVES[k], 1),
        )

    def back_copy(k):
        return remote(
            back.at[unit(k)],
            returned.at[unit(k)],
            back_send.at[k],
            back_recv.at[k],
            shift(position, MOVES[k], -1),
        )

    wide = base[...].astype(BF16).astype(F32)
    mean = jnp.mean(wide * wide, axis=-1, keepdims=True)
    normed = (wide * lax.rsqrt(mean + NORM_EPSILON) * gain[...]).astype(BF16)
    base[...] = wide
    part = width // PARTS
    stacked = jnp.concatenate([normed[:, q * part : (q + 1) * part] for q in range(PARTS)], axis=0)

    ids = index[...]
    relative = (
        ((((ids >> 5) - z) & 3) << 5)
        + ((((ids >> 3) - x) & 3) << 3)
        + ((((ids >> 1) - y) & 3) << 1)
        + ((ids - c) & 1)
    )
    experts = iota((LANES, rows), 0)
    chosen = jnp.zeros((LANES, rows), F32)
    scale = jnp.zeros((LANES, rows), F32)
    for k in range(ids.shape[0]):
        here = relative[k : k + 1, :] == experts
        chosen += jnp.where(here, 1.0, 0.0)
        scale += jnp.where(here, weights[k : k + 1, :], 0.0)
    chosen = nn(chosen.T.astype(BF16), slot_of[...])
    high, low = [nn(term, slot_of[...]).astype(BF16) for term in halves(scale.T)]
    earlier = jnp.where(iota((rows, rows), 0) > iota((rows, rows), 1), 1.0, 0.0).astype(BF16)
    rank = nn(earlier, chosen.astype(BF16))
    code = jnp.concatenate([(chosen * (rank + 1.0)).astype(BF16)] * PARTS, axis=0)
    high, low = [jnp.concatenate([term] * PARTS, axis=0) for term in (high, low)]

    groups = sent.shape[0] // GROUP
    per = GROUP // UNIT
    shape = (GROUP, PARTS * rows)
    place = iota(shape, 0) % UNIT
    fits = (place // SLOTS) == (iota(shape, 1) // rows)
    wanted = (place % SLOTS + 1).astype(F32)

    def select(k):
        found = (iota((GROUP, LANES), 0) + GROUP * k) // UNIT == iota((GROUP, LANES), 1)
        return jnp.where(found, 1.0, 0.0).astype(BF16)

    span = groups // CHUNKS

    def chunk_slots(k):
        return range(per * span * k, min(per * span * (k + 1), devices - 1))

    def launch(k):
        for slot in range(per * k, min(per * (k + 1), devices - 1)):
            out_copy(slot).start()

    for k in range(groups):
        found = nt(select(k), code)
        taken = jnp.where(fits & (found == wanted), 1.0, 0.0).astype(BF16)
        sent[GROUP * k : GROUP * (k + 1), :] = nn(taken, stacked).astype(BF16)
        if 0 < k <= WINDOW * span:
            launch(k - 1)
    if WINDOW * span >= groups:
        launch(groups - 1)
    arrived[unit(devices - 1), :] = sent[unit(devices - 1), :]

    for load in loads[3:5]:
        load.wait()
    gate_val = nn(normed, shared_gate_v[...])
    up_val = nn(normed, shared_up_v[...])
    shared = (gate_val * jax.nn.sigmoid(gate_val) * up_val).astype(BF16)
    loads[5].wait()
    for at in range(0, width, 512):
        base[:, at : at + 512] += nn(shared, shared_down_v[:, at : at + 512])

    shape = (PARTS * rows, GROUP)
    place = iota(shape, 1) % UNIT
    fits = (place // SLOTS) == (iota(shape, 0) // rows)
    wanted = (place % SLOTS + 1).astype(F32)
    for k in range(groups):
        chosen_here = select(k)
        match = fits & (nt(code, chosen_here) == wanted)
        match_high[k] = jnp.where(match, nt(high, chosen_here), 0.0).astype(BF16)
        match_low[k] = jnp.where(match, nt(low, chosen_here), 0.0).astype(BF16)

    a, b = iota((GROUP, GROUP), 0), iota((GROUP, GROUP), 1)
    here = (b % UNIT // SLOTS) * 64 + (b // UNIT) * SLOTS + b % SLOTS
    order = jnp.where(a == here, 1.0, 0.0).astype(BF16)
    there = (a % UNIT // SLOTS) * 64 + (a // UNIT) * SLOTS + a % SLOTS
    order_back = jnp.where(b == there, 1.0, 0.0).astype(BF16)
    for load in loads[6:]:
        load.wait()

    for chunk in range(CHUNKS):
        for slot in chunk_slots(chunk):
            out_copy(slot).wait_recv()
        for g in range(span):
            k = chunk * span + g
            sorted_ = nn(order, arrived[GROUP * k : GROUP * (k + 1), :]).astype(BF16)
            for q in range(PARTS):
                chunk_v[64 * g : 64 * (g + 1), q * part : (q + 1) * part] = sorted_[
                    64 * q : 64 * (q + 1)
                ]
        for at in range(0, hidden.shape[1], 256):
            gate_val = nn(chunk_v[...], gate_v[:, at : at + 256])
            up_val = nn(chunk_v[...], up_v[:, at : at + 256])
            hidden[:, at : at + 256] = (gate_val * jax.nn.sigmoid(gate_val) * up_val).astype(BF16)
        for at in range(0, width, 512):
            chunk_v[:, at : at + 512] = nn(hidden[...], down_v[:, at : at + 512]).astype(BF16)
        for g in range(span):
            k = chunk * span + g
            gathered = jnp.concatenate(
                [chunk_v[64 * g : 64 * (g + 1), q * part : (q + 1) * part] for q in range(PARTS)],
                axis=0,
            )
            back[GROUP * k : GROUP * (k + 1), :] = nn(order_back, gathered).astype(BF16)
        for slot in chunk_slots(chunk):
            back_copy(slot).start()
        if chunk + WINDOW < CHUNKS:
            for slot in chunk_slots(chunk):
                out_copy(slot).wait_send()
            for slot in chunk_slots(chunk + WINDOW):
                out_copy(slot).start()
    returned[unit(devices - 1), :] = back[unit(devices - 1), :]

    routed = jnp.zeros((PARTS * rows, part), F32)
    for k in range(groups):
        for slot in range(per * k, min(per * (k + 1), devices - 1)):
            back_copy(slot).wait_recv()
        block = returned[GROUP * k : GROUP * (k + 1), :]
        routed += nn(match_high[k], block) + nn(match_low[k], block)
    for q in range(PARTS):
        at = slice(q * part, (q + 1) * part)
        out[:, at] = (base[:, at] + routed[q * rows : (q + 1) * rows, :]).astype(BF16)
    for d in (2, 1, 3):

        @pl.when(z + d < 4)
        def _():
            col_copy(d).wait_send()

    for chunk in range(CHUNKS):
        for slot in chunk_slots(chunk):
            if chunk + WINDOW >= CHUNKS:
                out_copy(slot).wait_send()
            back_copy(slot).wait_send()


def slot_table():
    devices = len(MOVES)
    table = np.zeros((devices, devices), np.float32)
    for slot, (dz, dx, dy, dc) in enumerate(MOVES):
        table[((dz * 4 + dx) * 4 + dy) * 2 + dc, slot] = 1.0
    return jnp.asarray(table, BF16)


def layer_call(small, large):
    rows, width = large[0].shape
    long = small[0].shape[0]
    gate = large[3]
    devices = len(MOVES)
    part = width // PARTS
    slots = pltpu.VMEM((devices * UNIT, part), BF16)
    match = pltpu.VMEM((devices * UNIT // GROUP, PARTS * rows, GROUP), BF16)
    chunk_rows = devices * SLOTS // CHUNKS
    packed = (192, 2 * LANES)
    scratch = (
        [pltpu.VMEM((rows, width), BF16), pltpu.VMEM((2 * LANES, width), BF16)]
        + [pltpu.VMEM(a.shape, BF16) for a in large[3:]]
        + [
            pltpu.VMEM((2, long, LANES), F32),
            pltpu.VMEM((2, long, LANES), BF16),
            pltpu.VMEM((4, *packed), BF16),
            pltpu.VMEM((4, *packed), BF16),
            pltpu.VMEM(packed, BF16),
            pltpu.VMEM(packed, BF16),
            pltpu.VMEM((2, LANES, LANES), F32),
            pltpu.VMEM((4, rows, width), F32),
            pltpu.VMEM((4, rows, width), BF16),
            pltpu.VMEM((4, rows, width), BF16),
            pltpu.VMEM((6, rows, width // 2), BF16),
            pltpu.VMEM((6, rows, width // 2), BF16),
            pltpu.VMEM((rows, width), F32),
        ]
        + [slots] * 4
        + [
            pltpu.VMEM((chunk_rows, width), BF16),
            pltpu.VMEM((chunk_rows, gate.shape[1]), BF16),
            match,
            match,
            pltpu.SemaphoreType.DMA((9,)),
        ]
        + [pltpu.SemaphoreType.DMA((4,))] * 6
        + [pltpu.SemaphoreType.DMA((6,))] * 2
        + [pltpu.SemaphoreType.DMA((devices,))] * 4
    )
    return pl.pallas_call(
        layer_kernel,
        out_shape=jax.ShapeDtypeStruct((rows, width), BF16),
        in_specs=[pl.BlockSpec(memory_space=pltpu.VMEM)] * len(small)
        + [pl.BlockSpec(memory_space=pl.ANY)] * len(large),
        out_specs=pl.BlockSpec(memory_space=pltpu.VMEM),
        scratch_shapes=scratch,
        compiler_params=pltpu.CompilerParams(
            collective_id=0, has_side_effects=True, vmem_limit_bytes=60 * 1024 * 1024
        ),
        name="layer",
    )(*small, *large)


def local(
    residual,
    receptance_first,
    key_first_group,
    value_first_group,
    decay_preact_first,
    context_rate_first,
    decay_base_first,
    head_scale_first,
    receptance_second,
    key_second_group,
    value_second_group,
    decay_preact_second,
    context_rate_second,
    decay_base_second,
    head_scale_second,
    decay_extra_log,
    output_weight_first,
    output_weight_second,
    feedforward_gain,
    routed_expert_index,
    routed_expert_weight,
    expert_gate_weight,
    expert_up_weight,
    expert_down_weight,
    shared_gate_weight,
    shared_up_weight,
    shared_down_weight,
):
    small = (
        receptance_first,
        key_first_group,
        value_first_group,
        decay_preact_first,
        context_rate_first,
        decay_base_first[None, :],
        head_scale_first[None, :],
        receptance_second,
        key_second_group,
        value_second_group,
        decay_preact_second,
        context_rate_second,
        decay_base_second[None, :],
        head_scale_second[None, :],
        decay_extra_log.reshape(-1, SPAN),
        feedforward_gain[None, :],
        routed_expert_index.T,
        routed_expert_weight.T,
        slot_table(),
    )
    large = (
        residual,
        output_weight_first,
        output_weight_second,
        expert_gate_weight[0],
        expert_up_weight[0],
        expert_down_weight[0],
        shared_gate_weight,
        shared_up_weight,
        shared_down_weight,
    )
    return layer_call(small, large)


def solution(mesh):
    finer = Mesh(mesh.devices.reshape(4, 4, 4, 2), ALL)
    sp, tp = (Z, X), (Y, C)
    heads = (P(sp, tp),) * 5 + (P(tp),) * 2
    placed = (
        (P(ALL, None),)
        + heads
        + heads
        + (P(sp), P(tp, None), P(tp, None), P(), P(ALL, None), P(ALL, None))
        + (P(ALL, None, None),) * 3
        + (P(),) * 3
    )
    return jax.shard_map(
        local, mesh=finer, in_specs=placed, out_specs=P(ALL, None), check_vma=False
    )
```
